128 devices in a mesh: grp: 4 (over y, x), ep: 32 (over z, core).
Axes of the slice: x: 2, y: 2, z: 16, core: 2. Of those that a mesh axis runs over, the one named last changes fastest.
The devices are a block of a 8x8x16 slice.
Arguments:
- tokens: bfloat16 [512, 2048], P(('grp', 'ep')), parts along dimension 0, may hold values from -6 to 6
- memory_state: float32 [512, 4, 256, 512], P(('grp', 'ep')), parts along dimension 0, may hold values from -0.6 to 0.6
- max_state: float32 [512, 4], P(('grp', 'ep')), parts along dimension 0, may hold values from -4 to 4
- norm_gain: float32 [2048], replicated, may hold values from 0.1 to 1.9
- query_weight: bfloat16 [2048, 1024], P(None, 'ep'), may hold values from -0.125 to 0.125
- key_weight: bfloat16 [2048, 1024], P(None, 'ep'), may hold values from -0.125 to 0.125
- value_weight: bfloat16 [2048, 2048], P(None, 'ep'), may hold values from -0.125 to 0.125
- output_gate: bfloat16 [2048, 2048], P(None, 'ep'), may hold values from -0.125 to 0.125
- input_gate: bfloat16 [2048, 4], replicated, may hold values from -0.125 to 0.125
- forget_gate: bfloat16 [2048, 4], replicated, may hold values from -0.125 to 0.125
- forget_bias: float32 [4], replicated, may hold values from -2 to 4
- head_gain: float32 [2048], replicated, may hold values from 0.1 to 1.9
- output_weight: bfloat16 [2048, 2048], P(None, 'ep'), may hold values from -0.125 to 0.125
- expert_norm: float32 [2048], replicated, may hold values from 0.1 to 1.9
- routed_experts: int32 [512, 4], P(('grp', 'ep')), parts along dimension 0, may hold values from 0 to 31, as said below
- route_weights: float32 [512, 4], P(('grp', 'ep')), parts along dimension 0, may hold values from 0.1 to 1
- expert_gate: bfloat16 [32, 2048, 512], P('ep'), may hold values from -0.125 to 0.125
- expert_lift: bfloat16 [32, 2048, 512], P('ep'), may hold values from -0.125 to 0.125
- expert_down: bfloat16 [32, 512, 2048], P('ep'), may hold values from -0.25 to 0.25
Outputs:
- layer_out: bfloat16 [512, 2048], P(('grp', 'ep')), parts along dimension 0
- new_memory: float32 [512, 4, 256, 512], P(('grp', 'ep')), parts along dimension 0
- new_max: float32 [512, 4], P(('grp', 'ep')), parts along dimension 0
The draws below stay inside these ranges and needn't reach their ends.
There are 4 independent parts, one for each index of `grp`. The reference program is written for one: setup_inputs(seed, part) draws one part's arguments, and reference() takes and returns one part's arrays. A program takes and returns all parts, laid end to end along the dimension named above; an argument that names none is the same for every part. Nothing has to cross between parts.
Inputs may be any that keep to these rules, and one draw needn't show every extreme that they name: `routed_experts`: each row names 4 different experts of one group (expert e lies in group e // 8). No expert is named by more than 2 rows of one device, and some device has an expert named by 2 of its rows.
All inputs are finite; a program needn't handle non-finite values.
Results may differ from the reference program's by a relative error of at most 0.013.
Values may be sent and summed in bfloat16 or wider, within the bound.
No kernel may reach another device: no remote copies, remote signals or barrier semaphores. Data moves between devices by JAX's collectives and lax.ppermute only.
A program may use at most 64 MiB of HBM per device.

```python
import math
import jax
import jax.numpy as jnp
from jax import lax

D = 2048
HEADS = 4
DQK = 256
DV = 512
DE = 512
TOP = 4
GROUPS = 4
EXPERTS = 32
EPG = 8
SEQ_DEV = 4
SEQS = 128


def draw_routed_experts(key, part):
    base = jax.random.fold_in(key, 11)
    keys_all = jax.random.split(base, 4)
    device_count = SEQS // SEQ_DEV
    order = jax.random.permutation(keys_all[0], GROUPS)
    lowest = jnp.minimum(jax.random.randint(keys_all[1], (device_count,), 0, GROUPS), jax.random.randint(keys_all[2], (device_count,), 0, GROUPS))
    device_group = order[lowest]
    scores = jax.random.randint(keys_all[3], (device_count, EPG), 0, 1 << 20) * EPG + jnp.arange(EPG, dtype=jnp.int32)[None, :]
    shuffled = jnp.argsort(scores, axis=1).astype(jnp.int32)
    row_index = jnp.arange(SEQS, dtype=jnp.int32)
    device_of = row_index // SEQ_DEV
    pair_index = row_index % SEQ_DEV // 2
    halves = EPG // TOP
    slot_index = pair_index % (GROUPS * halves)
    group_ids = (device_group[device_of] + slot_index // halves) % GROUPS
    half_ids = slot_index % halves
    positions = half_ids[:, None] * TOP + jnp.arange(TOP, dtype=jnp.int32)[None, :]
    within = jnp.take_along_axis(shuffled[device_of], positions, axis=1)
    chosen = group_ids[:, None] * EPG + within
    return chosen.astype(jnp.int32)


def block_levels(key, dims, cuts, smallest, top_value):
    level, own = 1.0, jax.random.fold_in(key, 6)
    for dim, blocks in cuts:
        heights = jnp.exp(jax.random.uniform(jax.random.fold_in(own, dim), (blocks,), jnp.float32, smallest / len(cuts), top_value / len(cuts)))
        level = level * jnp.repeat(heights, dims[dim] // blocks).reshape([-1 if axis == dim else 1 for axis in range(len(dims))])
    return level


def noise(stream_key, dims, width, most, cuts=(), held_as=jnp.bfloat16):
    values = width * jax.random.normal(stream_key, dims, jnp.float32)
    if cuts:
        values = values * block_levels(stream_key, dims, cuts, -0.22, 0.18)
    return jnp.clip(values, -most, most).astype(held_as)


def setup_inputs(seed: int = 0, part: int = 0) -> dict:
    arg_keys = jax.random.split(jax.random.key(seed), 20)
    part_splits = jax.random.split(jax.random.fold_in(arg_keys[19], part), 20)
    tokens = noise(part_splits[0], (SEQS, D), 1.0, 6.0, ((0, 32),))
    memory_state = noise(part_splits[1], (SEQS, HEADS, DQK, DV), 0.1, 0.6, ((0, 32),), jnp.float32)
    max_state = noise(part_splits[2], (SEQS, HEADS), 1.0, 4.0, ((0, 32),), jnp.float32)
    norm_gain = jnp.clip(1.0 + 0.18 * jax.random.normal(arg_keys[3], (D,), jnp.float32), 0.1, 1.9)
    query_weight = noise(arg_keys[4], (D, HEADS * DQK), D ** -0.5, 0.125, ((1, 32),))
    key_weight = noise(arg_keys[5], (D, HEADS * DQK), D ** -0.5, 0.125, ((1, 32),))
    value_weight = noise(arg_keys[6], (D, HEADS * DV), D ** -0.5, 0.125, ((1, 32),))
    output_gate = noise(arg_keys[7], (D, HEADS * DV), D ** -0.5, 0.125, ((1, 32),))
    input_gate = noise(arg_keys[8], (D, HEADS), D ** -0.5, 0.125)
    forget_gate = noise(arg_keys[9], (D, HEADS), D ** -0.5, 0.125)
    forget_bias = jnp.clip(jax.random.uniform(arg_keys[10], (HEADS,), jnp.float32, -2.0, 4.0), -2.0, 4.0)
    head_gain = jnp.clip(1.0 + 0.18 * jax.random.normal(arg_keys[11], (HEADS * DV,), jnp.float32), 0.1, 1.9)
    output_weight = noise(arg_keys[12], (HEADS * DV, D), (HEADS * DV) ** -0.5, 0.125, ((1, 32),))
    expert_norm = jnp.clip(1.0 + 0.18 * jax.random.normal(arg_keys[13], (D,), jnp.float32), 0.1, 1.9)
    routed_experts = draw_routed_experts(jax.random.fold_in(jax.random.fold_in(arg_keys[19], part), 71), part)
    route_weights = jnp.clip(jnp.exp(math.log(1.0) - 2.3025851 * jax.random.uniform(part_splits[15], (SEQS, TOP), jnp.float32) ** block_levels(part_splits[15], (SEQS, TOP), ((0, 32),), -0.2, 0.2)), 0.1, 1.0)
    expert_gate = noise(arg_keys[16], (EXPERTS, D, DE), D ** -0.5, 0.125, ((0, 32),))
    expert_lift = noise(arg_keys[17], (EXPERTS, D, DE), D ** -0.5, 0.125, ((0, 32),))
    expert_down = noise(arg_keys[18], (EXPERTS, DE, D), DE ** -0.5, 0.25, ((0, 32),))
    return {"tokens": tokens, "memory_state": memory_state, "max_state": max_state, "norm_gain": norm_gain, "query_weight": query_weight, "key_weight": key_weight, "value_weight": value_weight, "output_gate": output_gate, "input_gate": input_gate, "forget_gate": forget_gate, "forget_bias": forget_bias, "head_gain": head_gain, "output_weight": output_weight, "expert_norm": expert_norm, "routed_experts": routed_experts, "route_weights": route_weights, "expert_gate": expert_gate, "expert_lift": expert_lift, "expert_down": expert_down}


epsilon = 1e-06

def scaled_norm(entries, gain):
    return entries * lax.rsqrt(lax.optimization_barrier(jnp.mean(entries * entries, axis=-1, keepdims=True)) + epsilon) * gain

def reference(tokens, memory_state, max_state, norm_gain, query_weight, key_weight, value_weight, output_gate, input_gate, forget_gate, forget_bias, head_gain, output_weight, expert_norm, routed_experts, route_weights, expert_gate, expert_lift, expert_down):
    seq_count = tokens.shape[0]
    inputs = tokens.astype(jnp.float32)
    normed = scaled_norm(inputs, norm_gain).astype(jnp.bfloat16)
    queries = jnp.dot(normed, query_weight, preferred_element_type=jnp.float32).astype(jnp.bfloat16)
    keys_proj = jnp.dot(normed, key_weight, preferred_element_type=jnp.float32).astype(jnp.bfloat16)
    values_proj = jnp.dot(normed, value_weight, preferred_element_type=jnp.float32).astype(jnp.bfloat16)
    gates = jnp.dot(normed, output_gate, preferred_element_type=jnp.float32).astype(jnp.bfloat16)
    input_logit = jnp.dot(normed, input_gate, preferred_element_type=jnp.float32)
    log_forget = jax.nn.log_sigmoid(jnp.dot(normed, forget_gate, preferred_element_type=jnp.float32) + forget_bias)
    query_heads = queries.astype(jnp.float32).reshape(seq_count, HEADS, DQK)
    key_heads = keys_proj.astype(jnp.float32).reshape(seq_count, HEADS, DQK) * DQK ** (-0.5)
    value_heads = values_proj.astype(jnp.float32).reshape(seq_count, HEADS, DV)
    new_max = jnp.maximum(log_forget + max_state, input_logit)
    carried = jnp.exp(log_forget + max_state - new_max)
    written = jnp.exp(input_logit - new_max)
    new_memory = carried[:, :, None, None] * memory_state + (written[:, :, None] * key_heads)[:, :, :, None] * value_heads[:, :, None, :]
    readout = jnp.einsum('shd,shde->she', query_heads, new_memory, precision=lax.Precision.HIGHEST)
    gate_heads = jax.nn.sigmoid(gates.astype(jnp.float32).reshape(seq_count, HEADS, DV))
    mixed = (scaled_norm(readout, head_gain.reshape(HEADS, DV)) * gate_heads).reshape(seq_count, HEADS * DV).astype(jnp.bfloat16)
    branch = jnp.dot(mixed, output_weight, preferred_element_type=jnp.float32).astype(jnp.bfloat16)
    residual = (inputs + branch.astype(jnp.float32)).astype(jnp.bfloat16)
    expert_in = scaled_norm(residual.astype(jnp.float32), expert_norm).astype(jnp.bfloat16)

    def one_token(packed):
        token_row, picked_experts, weights = packed
        token_float = token_row.astype(jnp.float32)
        gate_value = jnp.einsum('d,kdf->kf', token_float, expert_gate[picked_experts].astype(jnp.float32))
        lift_value = jnp.einsum('d,kdf->kf', token_float, expert_lift[picked_experts].astype(jnp.float32))
        hidden = (jax.nn.silu(gate_value) * lift_value).astype(jnp.bfloat16)
        expert_rows = jnp.einsum('kf,kfd->kd', hidden.astype(jnp.float32), expert_down[picked_experts].astype(jnp.float32)).astype(jnp.bfloat16)
        weighted = lax.optimization_barrier((weights[:, None] * expert_rows.astype(jnp.float32)).astype(jnp.bfloat16))
        return lax.optimization_barrier(jnp.sum(weighted.astype(jnp.float32), axis=0))
    expert_sum = lax.map(one_token, (expert_in, routed_experts, route_weights))
    layer_out = (residual.astype(jnp.float32) + expert_sum).astype(jnp.bfloat16)
    return (layer_out, new_memory, new_max)
```

```python
import jax
import jax.numpy as jnp
from jax import lax
from jax.sharding import PartitionSpec as P

epsilon = 1e-06


def scaled_norm(entries, gain):
    return entries * lax.rsqrt(jnp.mean(entries * entries, axis=-1, keepdims=True) + epsilon) * gain


def gather_blocks(block):
    size = lax.axis_size("ep")
    chips = size // 2
    core = lax.axis_index("ep") % 2
    same = lax.all_to_all(
        jnp.broadcast_to(block[None], (chips,) + block.shape),
        "ep",
        split_axis=0,
        concat_axis=0,
        tiled=True,
        axis_index_groups=[list(range(0, size, 2)), list(range(1, size, 2))],
    )
    other = lax.ppermute(same, "ep", [(i, i ^ 1) for i in range(size)])
    first = jnp.where(core == 0, same, other)
    second = jnp.where(core == 0, other, same)
    return jnp.stack([first, second], axis=1)


def body(
    tokens,
    memory_state,
    max_state,
    norm_gain,
    query_weight,
    key_weight,
    value_weight,
    output_gate,
    input_gate,
    forget_gate,
    forget_bias,
    head_gain,
    output_weight,
    expert_norm,
    routed_experts,
    route_weights,
    expert_gate,
    expert_lift,
    expert_down,
):
    seq_rows, width = tokens.shape
    head_count = forget_bias.shape[0]
    key_size = memory_state.shape[2]
    value_size = memory_state.shape[3]
    axis_size = lax.axis_size("ep")
    me = lax.axis_index("ep")
    all_rows = axis_size * seq_rows
    capacity = min(seq_rows, 2)
    f32, bf16 = jnp.float32, jnp.bfloat16

    token_rows = gather_blocks(tokens).reshape(all_rows, width)
    normed_rows = scaled_norm(token_rows.astype(f32), norm_gain).astype(bf16)
    tables = (query_weight, key_weight, value_weight, output_gate)
    widths = [table.shape[1] for table in tables]
    total = sum(widths)
    projected = jnp.concatenate(
        [jnp.dot(normed_rows, table, preferred_element_type=f32).astype(bf16) for table in tables],
        axis=1,
    ).reshape(axis_size, seq_rows, total)
    choices = routed_experts.shape[1]
    routing = jnp.broadcast_to(
        jnp.pad(routed_experts.astype(bf16), ((0, 0), (0, 64 - choices)))[None],
        (axis_size, seq_rows, 64),
    )
    received = lax.all_to_all(
        jnp.concatenate([projected, routing], axis=2), "ep", split_axis=0, concat_axis=0, tiled=True
    )
    pieces = []
    offset = 0
    for column_width in widths:
        pieces.append(
            received[:, :, offset : offset + column_width]
            .transpose(1, 0, 2)
            .reshape(seq_rows, axis_size * column_width)
        )
        offset = offset + column_width
    routed_all = received[:, :, offset : offset + choices].astype(jnp.int32).reshape(all_rows, choices)

    inputs = tokens.astype(f32)
    normed = scaled_norm(inputs, norm_gain).astype(bf16)
    query_heads = pieces[0].astype(f32).reshape(seq_rows, head_count, key_size)
    key_heads = pieces[1].astype(f32).reshape(seq_rows, head_count, key_size) * key_size ** (-0.5)
    value_heads = pieces[2].astype(f32).reshape(seq_rows, head_count, value_size)
    gate_heads = jax.nn.sigmoid(pieces[3].astype(f32).reshape(seq_rows, head_count, value_size))
    input_logit = jnp.dot(normed, input_gate, preferred_element_type=f32)
    log_forget = jax.nn.log_sigmoid(
        jnp.dot(normed, forget_gate, preferred_element_type=f32) + forget_bias
    )
    new_max = jnp.maximum(log_forget + max_state, input_logit)
    carried = jnp.exp(log_forget + max_state - new_max)
    written = jnp.exp(input_logit - new_max)
    new_memory = (
        carried[:, :, None, None] * memory_state
        + (written[:, :, None] * key_heads)[:, :, :, None] * value_heads[:, :, None, :]
    )
    readout = jnp.einsum("shd,shde->she", query_heads, new_memory, precision=lax.Precision.HIGHEST)
    mixed = (
        (scaled_norm(readout, head_gain.reshape(head_count, value_size)) * gate_heads)
        .reshape(seq_rows, width)
        .astype(bf16)
    )
    mixed_rows = gather_blocks(mixed).reshape(all_rows, width)
    columns = lax.dot_general(
        output_weight, mixed_rows, (((0,), (1,)), ((), ())), preferred_element_type=f32
    ).astype(bf16)
    branch_columns = gather_blocks(columns).reshape(width, all_rows)

    named = jnp.any(routed_all == me, axis=1).reshape(axis_size, seq_rows).astype(jnp.int32)
    slot = jnp.cumsum(named, axis=1) - named
    place = (jnp.arange(axis_size)[:, None] * capacity + slot).reshape(all_rows)
    wanted = jnp.where(named.reshape(all_rows) > 0, place, -1)
    slots = axis_size * capacity
    pick = (wanted[None, :] == jnp.arange(slots)[:, None])
    own = (me * seq_rows + jnp.arange(seq_rows))[:, None] == jnp.arange(all_rows)[None, :]
    pick = jnp.concatenate([pick, own], axis=0).astype(bf16)
    branch = lax.dot_general(
        pick, branch_columns, (((1,), (1,)), ((), ())), preferred_element_type=f32
    )
    picked_tokens = jnp.dot(pick, token_rows, preferred_element_type=f32)
    residual = (picked_tokens + branch).astype(bf16)
    own_residual = residual[slots:]
    expert_in = scaled_norm(residual[:slots].astype(f32), expert_norm).astype(bf16)
    hidden = (
        jax.nn.silu(jnp.dot(expert_in, expert_gate[0], preferred_element_type=f32))
        * jnp.dot(expert_in, expert_lift[0], preferred_element_type=f32)
    ).astype(bf16)
    results = (
        jnp.dot(hidden, expert_down[0], preferred_element_type=f32)
        .astype(bf16)
        .reshape(axis_size, capacity, width)
    )
    returned = lax.all_to_all(results, "ep", split_axis=0, concat_axis=0, tiled=True)
    expert_ids = jnp.arange(axis_size, dtype=jnp.int32)
    chosen = (routed_experts[:, :, None] == expert_ids[None, None, :]).astype(jnp.int32)
    present = jnp.sum(chosen, axis=1)
    before = jnp.cumsum(present, axis=0) - present
    slot_index = jnp.sum(chosen * before[:, None, :], axis=2)
    picked = returned.reshape(slots, width)[routed_experts * capacity + slot_index]
    weighted = lax.optimization_barrier(
        (route_weights[:, :, None] * picked.astype(f32)).astype(bf16)
    )
    expert_sum = jnp.sum(weighted.astype(f32), axis=1)
    layer_out = (own_residual.astype(f32) + expert_sum).astype(bf16)
    return (layer_out, new_memory, new_max)


def solution(mesh):
    return jax.shard_map(
        body,
        mesh=mesh,
        in_specs=(
            P(("grp", "ep"), None),
            P(("grp", "ep"), None, None, None),
            P(("grp", "ep"), None),
            P(),
            P(None, "ep"),
            P(None, "ep"),
            P(None, "ep"),
            P(None, "ep"),
            P(),
            P(),
            P(),
            P(),
            P(None, "ep"),
            P(),
            P(("grp", "ep"), None),
            P(("grp", "ep"), None),
            P("ep", None, None),
            P("ep", None, None),
            P("ep", None, None),
        ),
        out_specs=(
            P(("grp", "ep"), None),
            P(("grp", "ep"), None, None, None),
            P(("grp", "ep"), None),
        ),
        check_vma=False,
    )
```

```python
import jax
import jax.numpy as jnp
from jax import lax
from jax.experimental import pallas as pl
from jax.experimental.pallas import tpu as pltpu
from jax.sharding import PartitionSpec as P

epsilon = 1e-06
f32, bf16 = jnp.float32, jnp.bfloat16
lanes = 128
whole = pl.BlockSpec(memory_space=pltpu.VMEM)


def scaled_norm(entries, gain):
    return entries * lax.rsqrt(jnp.mean(entries * entries, axis=-1, keepdims=True) + epsilon) * gain


def exchange(blocks):
    size = lax.axis_size("ep")
    return lax.all_to_all(
        blocks,
        "ep",
        split_axis=0,
        concat_axis=0,
        tiled=True,
        axis_index_groups=[list(range(0, size, 2)), list(range(1, size, 2))],
    )


def spread(block):
    chips = lax.axis_size("ep") // 2
    return exchange(jnp.broadcast_to(block[None], (chips,) + block.shape))


def partner(block):
    return lax.ppermute(block, "ep", [(i, i ^ 1) for i in range(lax.axis_size("ep"))])


def project_kernel(rows, gain, table, out):
    entries = rows[...].astype(f32)
    normed = scaled_norm(entries, gain[...]).astype(bf16)
    out[...] = lax.dot_general(
        normed, table[...], (((1,), (1,)), ((), ())), preferred_element_type=f32
    ).astype(bf16)


def readout_kernel(chips, decayed, received, weight, gain, out, sums):
    seqs, heads, keys, values = decayed.shape
    per_head = chips // heads
    part = keys // per_head
    flat = received[...].astype(f32)
    pairs = flat[:, :lanes]
    columns = pairs.T
    for head in range(heads):
        for seq in range(seqs):
            total = jnp.zeros((8, values), f32)
            for j in range(per_head):
                at = (head * per_head + j) * seqs + seq
                block = decayed[seq, head, j * part : (j + 1) * part, :]
                terms = block * columns[:part, at : at + 1]
                total = total + jnp.sum(terms.reshape(part // 8, 8, values), axis=0)
            row = jnp.sum(total, axis=0, keepdims=True)
            for j in range(per_head):
                at = (head * per_head + j) * seqs + seq
                sums[at : at + 1, :] = row[:, j * lanes : (j + 1) * lanes]

    def head_total(entries):
        by_chip = entries.reshape(heads, per_head // 2, 2 * seqs, lanes)
        both = jnp.sum(by_chip, axis=1)
        both = both + jnp.concatenate([both[:, seqs:], both[:, :seqs]], axis=1)
        both = jnp.broadcast_to(both[:, None], by_chip.shape).reshape(entries.shape)
        return jnp.sum(both, axis=-1, keepdims=True)

    products = pairs * jnp.concatenate([pairs[:, part:], pairs[:, :part]], axis=1)
    match = head_total(products) * 0.5
    readout = sums[...] + (weight[...] * match) * flat[:, lanes : 2 * lanes]
    scale = lax.rsqrt(head_total(readout * readout) / values + epsilon)
    gates = jax.nn.sigmoid(flat[:, 2 * lanes : 3 * lanes])
    out[...] = (readout * scale * gain[...] * gates).astype(bf16)


def body(
    tokens,
    memory_state,
    max_state,
    norm_gain,
    query_weight,
    key_weight,
    value_weight,
    output_gate,
    input_gate,
    forget_gate,
    forget_bias,
    head_gain,
    output_weight,
    expert_norm,
    routed_experts,
    route_weights,
    expert_gate,
    expert_lift,
    expert_down,
):
    seq_rows, width = tokens.shape
    head_count = forget_bias.shape[0]
    key_size = memory_state.shape[2]
    value_size = memory_state.shape[3]
    axis_size = lax.axis_size("ep")
    chips = axis_size // 2
    me = lax.axis_index("ep")
    core = me % 2
    half_rows = chips * seq_rows
    capacity = min(seq_rows, 2)
    choices = routed_experts.shape[1]

    same_tokens = spread(tokens).reshape(half_rows, width)

    tables = []
    for table in (query_weight, key_weight, value_weight, output_gate, output_weight):
        mine = table.T
        theirs = partner(mine)
        tables.append(
            jnp.where(
                core == 0,
                jnp.concatenate([mine, theirs], axis=0),
                jnp.concatenate([theirs, mine], axis=0),
            )
        )
    table = jnp.concatenate(tables[:4], axis=0)
    total = table.shape[0]

    inputs = tokens.astype(f32)
    normed = scaled_norm(inputs, norm_gain).astype(bf16)
    input_logit = jnp.dot(normed, input_gate, preferred_element_type=f32)
    log_forget = jax.nn.log_sigmoid(
        jnp.dot(normed, forget_gate, preferred_element_type=f32) + forget_bias
    )
    new_max = jnp.maximum(log_forget + max_state, input_logit)
    carried = jnp.exp(log_forget + max_state - new_max)
    written = jnp.exp(input_logit - new_max) * key_size ** (-0.5)
    decayed = carried[:, :, None, None] * memory_state
    per_head = chips // head_count
    by_chip = (head_count, per_head, seq_rows, lanes)
    weight_rows = jnp.broadcast_to(written.T[:, None, :, None], by_chip).reshape(half_rows, lanes)
    gain_rows = jnp.broadcast_to(
        head_gain.reshape(head_count, per_head, 1, lanes), by_chip
    ).reshape(half_rows, lanes)
    same_tokens, table, decayed, weight_rows, gain_rows = lax.optimization_barrier(
        (same_tokens, table, decayed, weight_rows, gain_rows)
    )

    projected = pl.pallas_call(
        project_kernel,
        out_shape=jax.ShapeDtypeStruct((half_rows, total), bf16),
        in_specs=[whole] * 3,
        out_specs=whole,
        name="project",
    )(same_tokens, norm_gain[None], table)
    routing = jnp.pad(routed_experts.astype(bf16), ((0, 0), (0, lanes - choices)))
    received = exchange(
        jnp.concatenate(
            [
                projected.reshape(chips, seq_rows, total),
                jnp.broadcast_to(routing[None], (chips, seq_rows, lanes)),
            ],
            axis=2,
        )
    ).reshape(half_rows, total + lanes)

    mixed = pl.pallas_call(
        lambda *refs: readout_kernel(chips, *refs),
        out_shape=jax.ShapeDtypeStruct((half_rows, lanes), bf16),
        in_specs=[whole] * 4,
        out_specs=whole,
        scratch_shapes=[pltpu.VMEM((half_rows, lanes), f32)],
        compiler_params=pltpu.CompilerParams(vmem_limit_bytes=24 << 20),
        name="readout",
    )(decayed, received, weight_rows, gain_rows)
    mixed = mixed.reshape(chips, seq_rows, lanes).transpose(1, 0, 2).reshape(seq_rows, width)
    same_mixed = spread(mixed).reshape(half_rows, width)

    by_source = received.reshape(chips, seq_rows, total + lanes)
    edge = total // 6

    def own_columns(start, size):
        return (
            by_source[:, :, start : start + size]
            .transpose(1, 0, 2)
            .reshape(seq_rows, head_count, chips * size // head_count)
            .astype(f32)
        )

    key_heads = own_columns(edge, edge)
    value_heads = own_columns(2 * edge, 2 * edge)
    new_memory = (
        decayed + (written[:, :, None] * key_heads)[:, :, :, None] * value_heads[:, :, None, :]
    )

    columns = lax.dot_general(
        same_mixed, tables[4], (((1,), (1,)), ((), ())), preferred_element_type=f32
    ).astype(bf16)
    same_branch = spread(columns)
    other_branch = partner(same_branch)
    other_tokens = partner(same_tokens)

    same_routed = received[:, total : total + choices]
    other_routed = partner(received[:, total:])[:, :choices]
    same_named = jnp.any(same_routed == me.astype(bf16), axis=1).astype(jnp.int32)
    other_named = jnp.any(other_routed == me.astype(bf16), axis=1).astype(jnp.int32)
    named = jnp.stack([same_named, other_named]).reshape(2, chips, seq_rows)
    slot = jnp.cumsum(named, axis=2) - named
    source = 2 * jnp.arange(chips)[None, :, None] + jnp.stack([core, 1 - core])[:, None, None]
    place = jnp.where(named > 0, source * capacity + slot, -1).reshape(2 * half_rows)
    slots = axis_size * capacity
    pick = place[None, :] == jnp.arange(slots)[:, None]
    own = ((me // 2) * seq_rows + jnp.arange(seq_rows))[:, None] == jnp.arange(2 * half_rows)[None, :]
    pick = jnp.concatenate([pick, own], axis=0).astype(bf16)
    branch_rows = jnp.concatenate(
        [b.transpose(1, 0, 2).reshape(half_rows, width) for b in (same_branch, other_branch)], axis=0
    )
    token_rows = jnp.concatenate([same_tokens, other_tokens], axis=0)
    branch = jnp.dot(pick, branch_rows, preferred_element_type=f32)
    picked_tokens = jnp.dot(pick, token_rows, preferred_element_type=f32)
    residual = (picked_tokens + branch).astype(bf16)
    own_residual = residual[slots:]
    expert_in = scaled_norm(residual[:slots].astype(f32), expert_norm).astype(bf16)
    hidden = (
        jax.nn.silu(jnp.dot(expert_in, expert_gate[0], preferred_element_type=f32))
        * jnp.dot(expert_in, expert_lift[0], preferred_element_type=f32)
    ).astype(bf16)
    results = (
        jnp.dot(hidden, expert_down[0], preferred_element_type=f32)
        .astype(bf16)
        .reshape(axis_size, capacity, width)
    )
    returned = lax.all_to_all(results, "ep", split_axis=0, concat_axis=0, tiled=True)
    expert_ids = jnp.arange(axis_size, dtype=jnp.int32)
    chosen = (routed_experts[:, :, None] == expert_ids[None, None, :]).astype(jnp.int32)
    present = jnp.sum(chosen, axis=1)
    before = jnp.cumsum(present, axis=0) - present
    slot_index = jnp.sum(chosen * before[:, None, :], axis=2)
    picked = returned.reshape(slots, width)[routed_experts * capacity + slot_index]
    weighted = lax.optimization_barrier(
        (route_weights[:, :, None] * picked.astype(f32)).astype(bf16)
    )
    expert_sum = jnp.sum(weighted.astype(f32), axis=1)
    layer_out = (own_residual.astype(f32) + expert_sum).astype(bf16)
    return (layer_out, new_memory, new_max)
def solution(mesh):
    return jax.shard_map(
        body,
        mesh=mesh,
        in_specs=(
            P(("grp", "ep"), None),
            P(("grp", "ep"), None, None, None),
            P(("grp", "ep"), None),
            P(),
            P(None, "ep"),
            P(None, "ep"),
            P(None, "ep"),
            P(None, "ep"),
            P(),
            P(),
            P(),
            P(),
            P(None, "ep"),
            P(),
            P(("grp", "ep"), None),
            P(("grp", "ep"), None),
            P("ep", None, None),
            P("ep", None, None),
            P("ep", None, None),
        ),
        out_specs=(
            P(("grp", "ep"), None),
            P(("grp", "ep"), None, None, None),
            P(("grp", "ep"), None),
        ),
        check_vma=False,
    )
```

```python
import jax
import jax.numpy as jnp
from jax import lax
from jax.experimental import pallas as pl
from jax.experimental.pallas import tpu as pltpu
from jax.sharding import PartitionSpec as P

epsilon = 1e-06
f32, bf16 = jnp.float32, jnp.bfloat16
lanes = 128
whole = pl.BlockSpec(memory_space=pltpu.VMEM)


def scaled_norm(entries, gain):
    return entries * lax.rsqrt(jnp.mean(entries * entries, axis=-1, keepdims=True) + epsilon) * gain


def exchange(blocks):
    size = lax.axis_size("ep")
    return lax.all_to_all(
        blocks,
        "ep",
        split_axis=0,
        concat_axis=0,
        tiled=True,
        axis_index_groups=[list(range(0, size, 2)), list(range(1, size, 2))],
    )


def spread(block):
    chips = lax.axis_size("ep") // 2
    return exchange(jnp.broadcast_to(block[None], (chips,) + block.shape))


def partner(block):
    return lax.ppermute(block, "ep", [(i, i ^ 1) for i in range(lax.axis_size("ep"))])


def gate_kernel(key_size, tokens, gain, in_table, forget_table, bias, last_max, head_gain, new_max, carried, written, carried_rows, weight_rows, gain_rows):
    seqs = tokens.shape[0]
    heads, chips = bias.shape[1], head_gain.shape[0]
    normed = scaled_norm(tokens[...].astype(f32), gain[...]).astype(bf16)

    def logits(table):
        return lax.dot_general(
            normed, table[...], (((1,), (1,)), ((), ())), preferred_element_type=f32
        )

    input_logit = logits(in_table)
    forget_logit = logits(forget_table) + bias[...]
    log_forget = jnp.minimum(forget_logit, 0.0) - jnp.log1p(jnp.exp(-jnp.abs(forget_logit)))
    shifted = log_forget + last_max[...]
    top = jnp.maximum(shifted, input_logit)
    weight = jnp.exp(input_logit - top) * key_size ** (-0.5)
    kept = jnp.exp(shifted - top)
    new_max[...] = top
    carried[...] = kept
    written[...] = weight
    for chip in range(chips):
        head = chip // (chips // heads)
        rows = pl.ds(chip * seqs, seqs)
        carried_rows[rows, :] = jnp.broadcast_to(kept[:, head : head + 1], (seqs, lanes))
        weight_rows[rows, :] = jnp.broadcast_to(weight[:, head : head + 1], (seqs, lanes))
        gain_rows[rows, :] = jnp.broadcast_to(head_gain[chip : chip + 1, :], (seqs, lanes))


def gather_tables(core, tables, out):
    start = 0
    for mine, theirs in zip(tables[::2], tables[1::2]):
        count = mine.shape[0]
        own = pl.multiple_of(start + core[0] * count, count)
        other = pl.multiple_of(start + (1 - core[0]) * count, count)
        out[pl.ds(own, count), :] = mine[...]
        out[pl.ds(other, count), :] = theirs[...]
        start += 2 * count


def project_kernel(core, blocks, gain, routing, *refs):
    tables, (out, table, rows) = refs[:-3], refs[-3:]
    chips, seqs = blocks.shape[:2]
    gather_tables(core, tables, table)
    for chip in range(chips):
        rows[chip * seqs : (chip + 1) * seqs, :] = blocks[chip].astype(f32)
    normed = scaled_norm(rows[...], gain[...]).astype(bf16)
    columns = lax.dot_general(
        normed, table[...], (((1,), (1,)), ((), ())), preferred_element_type=f32
    )
    total = columns.shape[1]
    for chip in range(chips):
        out[chip, :, :total] = columns[chip * seqs : (chip + 1) * seqs, :].astype(bf16)
        out[chip, :, total:] = routing[...]


def mix_kernel(core, blocks, mine, theirs, out, table, rows):
    chips, seqs = blocks.shape[:2]
    gather_tables(core, (mine, theirs), table)
    for chip in range(chips):
        rows[chip * seqs : (chip + 1) * seqs, :] = blocks[chip].astype(f32)
    columns = lax.dot_general(
        rows[...].astype(bf16), table[...], (((1,), (1,)), ((), ())), preferred_element_type=f32
    ).astype(bf16)
    for chip in range(chips):
        out[chip] = columns


def readout_kernel(state, received, carried, weight, gain, out, sums, flat, memory, arrived):
    seqs, heads, keys, values = state.shape
    chips = received.shape[0]
    per_head = chips // heads
    part = keys // per_head
    copies = {}
    for head in range(heads):
        for seq in range(seqs):
            copies[head, seq] = pltpu.make_async_copy(
                state.at[seq, head], memory.at[seq, head], arrived.at[seq, head]
            )
            copies[head, seq].start()
    for chip in range(chips):
        flat[chip * seqs : (chip + 1) * seqs, :] = received[chip].astype(f32)
    pairs = flat[:, :lanes]
    columns = pairs.T
    for head in range(heads):
        for seq in range(seqs):
            copies[head, seq].wait()
            total = jnp.zeros((8, values), f32)
            for j in range(per_head):
                at = (head * per_head + j) * seqs + seq
                block = memory[seq, head, j * part : (j + 1) * part, :]
                terms = block * columns[:part, at : at + 1]
                total = total + jnp.sum(terms.reshape(part // 8, 8, values), axis=0)
            row = jnp.sum(total, axis=0, keepdims=True)
            for j in range(per_head):
                at = (head * per_head + j) * seqs + seq
                sums[at : at + 1, :] = row[:, j * lanes : (j + 1) * lanes]

    def head_total(entries):
        by_chip = entries.reshape(heads, per_head // 2, 2 * seqs, lanes)
        both = jnp.sum(by_chip, axis=1)
        both = both + jnp.concatenate([both[:, seqs:], both[:, :seqs]], axis=1)
        both = jnp.broadcast_to(both[:, None], by_chip.shape).reshape(entries.shape)
        return jnp.sum(both, axis=-1, keepdims=True)

    products = pairs * jnp.concatenate([pairs[:, part:], pairs[:, :part]], axis=1)
    match = head_total(products) * 0.5
    readout = carried[...] * sums[...] + (weight[...] * match) * flat[:, lanes : 2 * lanes]
    scale = lax.rsqrt(head_total(readout * readout) / values + epsilon)
    gates = jax.nn.sigmoid(flat[:, 2 * lanes : 3 * lanes])
    mixed = readout * scale * gain[...] * gates
    for chip in range(chips):
        tile = mixed[chip * seqs : (chip + 1) * seqs, :].astype(bf16)
        for copy in range(chips):
            out[copy, :, chip * lanes : (chip + 1) * lanes] = tile


def body(
    tokens,
    memory_state,
    max_state,
    norm_gain,
    query_weight,
    key_weight,
    value_weight,
    output_gate,
    input_gate,
    forget_gate,
    forget_bias,
    head_gain,
    output_weight,
    expert_norm,
    routed_experts,
    route_weights,
    expert_gate,
    expert_lift,
    expert_down,
):
    seq_rows, width = tokens.shape
    head_count = forget_bias.shape[0]
    key_size = memory_state.shape[2]
    value_size = memory_state.shape[3]
    axis_size = lax.axis_size("ep")
    chips = axis_size // 2
    me = lax.axis_index("ep")
    core = me % 2
    half_rows = chips * seq_rows
    capacity = min(seq_rows, 2)
    choices = routed_experts.shape[1]

    same_tokens = spread(tokens)

    pairs = []
    for table in (query_weight, key_weight, value_weight, output_gate, output_weight):
        pairs += [table.T, partner(table.T)]
    total = sum(table.shape[0] for table in pairs[:-2])

    per_head = chips // head_count
    gate_shape = jax.ShapeDtypeStruct((seq_rows, head_count), f32)
    row_shape = jax.ShapeDtypeStruct((half_rows, lanes), f32)
    new_max, carried, written, carried_rows, weight_rows, gain_rows = pl.pallas_call(
        lambda *refs: gate_kernel(key_size, *refs),
        out_shape=(gate_shape,) * 3 + (row_shape,) * 3,
        in_specs=[whole] * 7,
        out_specs=(whole,) * 6,
        compiler_params=pltpu.CompilerParams(vmem_limit_bytes=4 << 20),
        name="gates",
    )(
        tokens,
        norm_gain[None],
        input_gate.T,
        forget_gate.T,
        forget_bias[None],
        max_state,
        head_gain.reshape(chips, lanes),
    )
    routing = jnp.pad(routed_experts.astype(bf16), ((0, 0), (0, lanes - choices)))
    same_tokens, pairs, carried_rows, weight_rows, gain_rows, routing = lax.optimization_barrier(
        (same_tokens, pairs, carried_rows, weight_rows, gain_rows, routing)
    )

    scalar = pl.BlockSpec(memory_space=pltpu.SMEM)
    received = exchange(
        pl.pallas_call(
            project_kernel,
            out_shape=jax.ShapeDtypeStruct((chips, seq_rows, total + lanes), bf16),
            in_specs=[scalar] + [whole] * (1 + len(pairs)),
            out_specs=whole,
            scratch_shapes=[pltpu.VMEM((total, width), bf16), pltpu.VMEM((half_rows, width), f32)],
            compiler_params=pltpu.CompilerParams(vmem_limit_bytes=8 << 20),
            name="project",
        )(core[None], same_tokens, norm_gain[None], routing, *pairs[:-2])
    )
    same_mixed = exchange(
        pl.pallas_call(
            readout_kernel,
            out_shape=jax.ShapeDtypeStruct((chips, seq_rows, width), bf16),
            in_specs=[pl.BlockSpec(memory_space=pltpu.HBM)] + [whole] * 4,
            out_specs=whole,
            scratch_shapes=[
                pltpu.VMEM((half_rows, lanes), f32),
                pltpu.VMEM((half_rows, total + lanes), f32),
                pltpu.VMEM(memory_state.shape, f32),
                pltpu.SemaphoreType.DMA(memory_state.shape[:2]),
            ],
            compiler_params=pltpu.CompilerParams(vmem_limit_bytes=48 << 20),
            name="readout",
        )(memory_state, received, carried_rows, weight_rows, gain_rows)
    )

    by_source = received
    edge = total // 6

    def own_columns(start, size):
        return (
            by_source[:, :, start : start + size]
            .transpose(1, 0, 2)
            .reshape(seq_rows, head_count, chips * size // head_count)
            .astype(f32)
        )

    key_heads = own_columns(edge, edge)
    value_heads = own_columns(2 * edge, 2 * edge)
    new_memory = (
        carried[:, :, None, None] * memory_state
        + (written[:, :, None] * key_heads)[:, :, :, None] * value_heads[:, :, None, :]
    )

    same_branch = exchange(
        pl.pallas_call(
            mix_kernel,
            out_shape=jax.ShapeDtypeStruct((chips, half_rows, lanes), bf16),
            in_specs=[scalar] + [whole] * 3,
            out_specs=whole,
            scratch_shapes=[pltpu.VMEM((lanes, width), bf16), pltpu.VMEM((half_rows, width), f32)],
            compiler_params=pltpu.CompilerParams(vmem_limit_bytes=4 << 20),
            name="mix",
        )(core[None], same_mixed, *pairs[-2:])
    )
    other_branch = partner(same_branch)
    other_tokens = partner(same_tokens)

    same_tokens = same_tokens.reshape(half_rows, width)
    other_tokens = other_tokens.reshape(half_rows, width)
    same_routed = received[:, :, total:]
    other_routed = partner(same_routed).reshape(half_rows, lanes)[:, :choices]
    same_routed = same_routed.reshape(half_rows, lanes)[:, :choices]
    same_named = jnp.any(same_routed == me.astype(bf16), axis=1).astype(jnp.int32)
    other_named = jnp.any(other_routed == me.astype(bf16), axis=1).astype(jnp.int32)
    named = jnp.stack([same_named, other_named]).reshape(2, chips, seq_rows)
    slot = jnp.cumsum(named, axis=2) - named
    source = 2 * jnp.arange(chips)[None, :, None] + jnp.stack([core, 1 - core])[:, None, None]
    place = jnp.where(named > 0, source * capacity + slot, -1).reshape(2 * half_rows)
    slots = axis_size * capacity
    pick = place[None, :] == jnp.arange(slots)[:, None]
    own = ((me // 2) * seq_rows + jnp.arange(seq_rows))[:, None] == jnp.arange(2 * half_rows)[None, :]
    pick = jnp.concatenate([pick, own], axis=0).astype(bf16)
    branch_rows = jnp.concatenate(
        [b.transpose(1, 0, 2).reshape(half_rows, width) for b in (same_branch, other_branch)], axis=0
    )
    token_rows = jnp.concatenate([same_tokens, other_tokens], axis=0)
    branch = jnp.dot(pick, branch_rows, preferred_element_type=f32)
    picked_tokens = jnp.dot(pick, token_rows, preferred_element_type=f32)
    residual = (picked_tokens + branch).astype(bf16)
    own_residual = residual[slots:]
    expert_in = scaled_norm(residual[:slots].astype(f32), expert_norm).astype(bf16)
    hidden = (
        jax.nn.silu(jnp.dot(expert_in, expert_gate[0], preferred_element_type=f32))
        * jnp.dot(expert_in, expert_lift[0], preferred_element_type=f32)
    ).astype(bf16)
    results = (
        jnp.dot(hidden, expert_down[0], preferred_element_type=f32)
        .astype(bf16)
        .reshape(axis_size, capacity, width)
    )
    routed_experts, results = lax.optimization_barrier((routed_experts, results))
    returned = lax.all_to_all(results, "ep", split_axis=0, concat_axis=0, tiled=True)
    expert_ids = jnp.arange(axis_size, dtype=jnp.int32)
    chosen = (routed_experts[:, :, None] == expert_ids[None, None, :]).astype(jnp.int32)
    present = jnp.sum(chosen, axis=1)
    before = jnp.cumsum(present, axis=0) - present
    slot_index = jnp.sum(chosen * before[:, None, :], axis=2)
    picked = returned.reshape(slots, width)[routed_experts * capacity + slot_index]
    weighted = lax.optimization_barrier(
        (route_weights[:, :, None] * picked.astype(f32)).astype(bf16)
    )
    expert_sum = jnp.sum(weighted.astype(f32), axis=1)
    layer_out = (own_residual.astype(f32) + expert_sum).astype(bf16)
    return (layer_out, new_memory, new_max)
def solution(mesh):
    return jax.shard_map(
        body,
        mesh=mesh,
        in_specs=(
            P(("grp", "ep"), None),
            P(("grp", "ep"), None, None, None),
            P(("grp", "ep"), None),
            P(),
            P(None, "ep"),
            P(None, "ep"),
            P(None, "ep"),
            P(None, "ep"),
            P(),
            P(),
            P(),
            P(),
            P(None, "ep"),
            P(),
            P(("grp", "ep"), None),
            P(("grp", "ep"), None),
            P("ep", None, None),
            P("ep", None, None),
            P("ep", None, None),
        ),
        out_specs=(
            P(("grp", "ep"), None),
            P(("grp", "ep"), None, None, None),
            P(("grp", "ep"), None),
        ),
        check_vma=False,
    )
```

```python
import jax
import jax.numpy as jnp
from jax import lax
from jax.experimental import pallas as pl
from jax.experimental.pallas import tpu as pltpu
from jax.sharding import PartitionSpec as P

epsilon = 1e-06
f32, bf16 = jnp.float32, jnp.bfloat16
lanes = 128
whole = pl.BlockSpec(memory_space=pltpu.VMEM)
hbm = pl.BlockSpec(memory_space=pltpu.HBM)
scalar = pl.BlockSpec(memory_space=pltpu.SMEM)


def in_hbm(array):
    return pltpu.with_memory_space_constraint(array, pltpu.HBM)


def scaled_norm(entries, gain):
    return entries * lax.rsqrt(jnp.mean(entries * entries, axis=-1, keepdims=True) + epsilon) * gain


def exchange(blocks):
    size = lax.axis_size("ep")
    return lax.all_to_all(
        blocks,
        "ep",
        split_axis=0,
        concat_axis=0,
        tiled=True,
        axis_index_groups=[list(range(0, size, 2)), list(range(1, size, 2))],
    )


def spread(block):
    chips = lax.axis_size("ep") // 2
    return exchange(jnp.broadcast_to(block[None], (chips,) + block.shape))


def partner(block):
    return lax.ppermute(block, "ep", [(i, i ^ 1) for i in range(lax.axis_size("ep"))])


def gate_kernel(key_size, tokens, gain, in_table, forget_table, bias, last_max, head_gain, new_max, carried, written, carried_rows, weight_rows, gain_rows):
    seqs = tokens.shape[0]
    heads, chips = bias.shape[1], head_gain.shape[0]
    normed = scaled_norm(tokens[...].astype(f32), gain[...]).astype(bf16)

    def logits(table):
        return lax.dot_general(
            normed, table[...], (((1,), (1,)), ((), ())), preferred_element_type=f32
        )

    input_logit = logits(in_table)
    forget_logit = logits(forget_table) + bias[...]
    log_forget = jnp.minimum(forget_logit, 0.0) - jnp.log1p(jnp.exp(-jnp.abs(forget_logit)))
    shifted = log_forget + last_max[...]
    top = jnp.maximum(shifted, input_logit)
    weight = jnp.exp(input_logit - top) * key_size ** (-0.5)
    kept = jnp.exp(shifted - top)
    new_max[...] = top
    carried[...] = kept
    written[...] = weight
    for chip in range(chips):
        head = chip // (chips // heads)
        rows = pl.ds(chip * seqs, seqs)
        carried_rows[rows, :] = jnp.broadcast_to(kept[:, head : head + 1], (seqs, lanes))
        weight_rows[rows, :] = jnp.broadcast_to(weight[:, head : head + 1], (seqs, lanes))
        gain_rows[rows, :] = jnp.broadcast_to(head_gain[chip : chip + 1, :], (seqs, lanes))


def place_tables(core, tables):
    start = 0
    for mine, theirs in zip(tables[::2], tables[1::2]):
        count = mine.shape[0]
        yield mine, pl.ds(pl.multiple_of(start + core[0] * count, count), count)
        yield theirs, pl.ds(pl.multiple_of(start + (1 - core[0]) * count, count), count)
        start += 2 * count


def project_kernel(core, blocks, routing, norm_gain, *refs):
    tables, (out, table, rows, gain, arrived) = refs[:-5], refs[-5:]
    chips, seqs = blocks.shape[:2]
    copies = [
        pltpu.make_async_copy(source, table.at[where], arrived.at[i])
        for i, (source, where) in enumerate(place_tables(core, tables))
    ]
    copies.append(pltpu.make_async_copy(norm_gain, gain, arrived.at[len(tables)]))
    for copy in copies:
        copy.start()
    for chip in range(chips):
        rows[chip * seqs : (chip + 1) * seqs, :] = blocks[chip].astype(f32)
    for copy in copies:
        copy.wait()
    normed = scaled_norm(rows[...], gain[...]).astype(bf16)
    columns = lax.dot_general(
        normed, table[...], (((1,), (1,)), ((), ())), preferred_element_type=f32
    )
    total = columns.shape[1]
    for chip in range(chips):
        out[chip, :, :total] = columns[chip * seqs : (chip + 1) * seqs, :].astype(bf16)
        out[chip, :, total:] = routing[...]


def mix_kernel(core, blocks, mine, theirs, out, table, rows):
    chips, seqs = blocks.shape[:2]
    for source, where in place_tables(core, (mine, theirs)):
        table[where, :] = source[...]
    for chip in range(chips):
        rows[chip * seqs : (chip + 1) * seqs, :] = blocks[chip].astype(f32)
    columns = lax.dot_general(
        rows[...].astype(bf16), table[...], (((1,), (1,)), ((), ())), preferred_element_type=f32
    ).astype(bf16)
    for chip in range(chips):
        out[chip] = columns


def readout_kernel(state, received, carried, weight, gain, out, sums, flat, memory, arrived):
    seqs, heads, keys, values = state.shape
    chips = received.shape[0]
    per_head = chips // heads
    part = keys // per_head
    copies = {}
    for head in range(heads):
        for seq in range(seqs):
            copies[head, seq] = pltpu.make_async_copy(
                state.at[seq, head], memory.at[seq, head], arrived.at[seq, head]
            )
            copies[head, seq].start()
    for chip in range(chips):
        flat[chip * seqs : (chip + 1) * seqs, :] = received[chip].astype(f32)
    pairs = flat[:, :lanes]
    columns = pairs.T
    for head in range(heads):
        for seq in range(seqs):
            copies[head, seq].wait()
            total = jnp.zeros((8, values), f32)
            for j in range(per_head):
                at = (head * per_head + j) * seqs + seq
                block = memory[seq, head, j * part : (j + 1) * part, :]
                terms = block * columns[:part, at : at + 1]
                total = total + jnp.sum(terms.reshape(part // 8, 8, values), axis=0)
            row = jnp.sum(total, axis=0, keepdims=True)
            for j in range(per_head):
                at = (head * per_head + j) * seqs + seq
                sums[at : at + 1, :] = row[:, j * lanes : (j + 1) * lanes]

    def head_total(entries):
        by_chip = entries.reshape(heads, per_head // 2, 2 * seqs, lanes)
        both = jnp.sum(by_chip, axis=1)
        both = both + jnp.concatenate([both[:, seqs:], both[:, :seqs]], axis=1)
        both = jnp.broadcast_to(both[:, None], by_chip.shape).reshape(entries.shape)
        return jnp.sum(both, axis=-1, keepdims=True)

    products = pairs * jnp.concatenate([pairs[:, part:], pairs[:, :part]], axis=1)
    match = head_total(products) * 0.5
    readout = carried[...] * sums[...] + (weight[...] * match) * flat[:, lanes : 2 * lanes]
    scale = lax.rsqrt(head_total(readout * readout) / values + epsilon)
    gates = jax.nn.sigmoid(flat[:, 2 * lanes : 3 * lanes])
    mixed = readout * scale * gain[...] * gates
    for chip in range(chips):
        tile = mixed[chip * seqs : (chip + 1) * seqs, :].astype(bf16)
        for copy in range(chips):
            out[copy, :, chip * lanes : (chip + 1) * lanes] = tile


def pick_kernel(me, same_routed, other_routed, same_tokens, other_tokens, pick, picked, routed, rows):
    chips, seqs = same_tokens.shape[:2]
    half = chips * seqs
    core = me[0] % 2
    for chip in range(chips):
        at = chip * seqs
        routed[at : at + seqs, :] = same_routed[chip].astype(f32)
        routed[half + at : half + at + seqs, :] = other_routed[chip].astype(f32)
        rows[at : at + seqs, :] = same_tokens[chip].astype(f32)
        rows[half + at : half + at + seqs, :] = other_tokens[chip].astype(f32)
    choices = routed[...].T[:8]
    valid = lax.broadcasted_iota(jnp.int32, choices.shape, 0) < seqs
    hits = jnp.where(valid & (choices == me[0].astype(f32)), 1.0, 0.0)
    named = jnp.broadcast_to(jnp.sum(hits, axis=0, keepdims=True), hits.shape)
    lane = lax.broadcasted_iota(jnp.int32, hits.shape, 1)
    slot = jnp.zeros(hits.shape, f32)
    for back in range(1, seqs):
        slot = slot + jnp.where(lane % seqs >= back, pltpu.roll(named, back, 1), 0.0)
    source = 2 * (lane % half // seqs) + jnp.where(lane < half, core, 1 - core)
    place = jnp.where(named > 0.0, 2 * source + slot.astype(jnp.int32), -1)
    index = lax.broadcasted_iota(jnp.int32, pick.shape, 0)
    slots = 4 * chips
    mine = lax.broadcasted_iota(jnp.int32, pick.shape, 1) + slots - me[0] // 2 * seqs
    wanted = jnp.where(index < slots, jnp.broadcast_to(place[:1], pick.shape), mine)
    chosen = jnp.where(wanted == index, 1.0, 0.0).astype(bf16)
    pick[...] = chosen
    picked[...] = jnp.dot(chosen, rows[...].astype(bf16), preferred_element_type=f32).astype(bf16)


def expert_kernel(pick, tokens, same, other, gain, gate, lift, down, out, own, branch, *refs):
    gate_table, lift_table, down_table, arrived = refs
    copies = [
        pltpu.make_async_copy(source.at[0], target, arrived.at[i])
        for i, (source, target) in enumerate(
            ((gate, gate_table), (lift, lift_table), (down, down_table))
        )
    ]
    for copy in copies:
        copy.start()
    chips, rows = same.shape[:2]
    for chip in range(chips):
        columns = slice(chip * lanes, (chip + 1) * lanes)
        branch[:rows, columns] = same[chip]
        branch[rows:, columns] = other[chip]
    added = jnp.dot(pick[...], branch[...], preferred_element_type=f32)
    residual = (tokens[...].astype(f32) + added).astype(bf16)
    devices, capacity = out.shape[:2]
    slots = devices * capacity
    own[...] = residual[slots:][: own.shape[0]]
    expert_in = scaled_norm(residual[:slots].astype(f32), gain[...]).astype(bf16)
    copies[0].wait()
    gate_value = jnp.dot(expert_in, gate_table[...], preferred_element_type=f32)
    copies[1].wait()
    lift_value = jnp.dot(expert_in, lift_table[...], preferred_element_type=f32)
    hidden = (jax.nn.silu(gate_value) * lift_value).astype(bf16)
    copies[2].wait()
    results = jnp.dot(hidden, down_table[...], preferred_element_type=f32)
    for device in range(devices):
        out[device] = results[device * capacity : (device + 1) * capacity, :].astype(bf16)


def combine_kernel(expert, slot, weights, returned, own, out):
    seqs, choices = weights.shape
    for seq in range(seqs):
        total = jnp.zeros((1, out.shape[1]), f32)
        for choice in range(choices):
            pair = returned[expert[seq, choice]].astype(f32)
            row = pair[:1]
            for other in range(1, pair.shape[0]):
                row = jnp.where(slot[seq, choice] == other, pair[other : other + 1], row)
            total = total + (weights[seq, choice] * row).astype(bf16).astype(f32)
        out[seq : seq + 1, :] = (own[seq : seq + 1, :].astype(f32) + total).astype(bf16)


def body(
    tokens,
    memory_state,
    max_state,
    norm_gain,
    query_weight,
    key_weight,
    value_weight,
    output_gate,
    input_gate,
    forget_gate,
    forget_bias,
    head_gain,
    output_weight,
    expert_norm,
    routed_experts,
    route_weights,
    expert_gate,
    expert_lift,
    expert_down,
):
    seq_rows, width = tokens.shape
    head_count = forget_bias.shape[0]
    key_size = memory_state.shape[2]
    value_size = memory_state.shape[3]
    axis_size = lax.axis_size("ep")
    chips = axis_size // 2
    me = lax.axis_index("ep")
    core = me % 2
    half_rows = chips * seq_rows
    capacity = min(seq_rows, 2)
    choices = routed_experts.shape[1]

    same_tokens = spread(tokens)

    pairs = []
    for table in (query_weight, key_weight, value_weight, output_gate, output_weight):
        pairs += [table.T, partner(table.T)]
    total = sum(table.shape[0] for table in pairs[:-2])

    per_head = chips // head_count
    gate_shape = jax.ShapeDtypeStruct((seq_rows, head_count), f32)
    row_shape = jax.ShapeDtypeStruct((half_rows, lanes), f32)
    new_max, carried, written, carried_rows, weight_rows, gain_rows = pl.pallas_call(
        lambda *refs: gate_kernel(key_size, *refs),
        out_shape=(gate_shape,) * 3 + (row_shape,) * 3,
        in_specs=[whole] * 7,
        out_specs=(whole,) * 6,
        compiler_params=pltpu.CompilerParams(vmem_limit_bytes=4 << 20),
        name="gates",
    )(
        tokens,
        norm_gain[None],
        input_gate.T,
        forget_gate.T,
        forget_bias[None],
        max_state,
        head_gain.reshape(chips, lanes),
    )
    routing = jnp.pad(routed_experts.astype(bf16), ((0, 0), (0, lanes - choices)))
    same_tokens, pairs, carried_rows, weight_rows, gain_rows, routing = lax.optimization_barrier(
        (same_tokens, pairs, carried_rows, weight_rows, gain_rows, routing)
    )

    received = exchange(
        pl.pallas_call(
            project_kernel,
            out_shape=jax.ShapeDtypeStruct((chips, seq_rows, total + lanes), bf16),
            in_specs=[scalar] + [whole] * 2 + [hbm] * (len(pairs) - 1),
            out_specs=whole,
            scratch_shapes=[
                pltpu.VMEM((total, width), bf16),
                pltpu.VMEM((half_rows, width), f32),
                pltpu.VMEM((1, width), f32),
                pltpu.SemaphoreType.DMA((len(pairs) - 1,)),
            ],
            compiler_params=pltpu.CompilerParams(vmem_limit_bytes=8 << 20),
            name="project",
        )(core[None], same_tokens, routing, *map(in_hbm, [norm_gain[None]] + pairs[:-2]))
    )
    same_mixed = exchange(
        pl.pallas_call(
            readout_kernel,
            out_shape=jax.ShapeDtypeStruct((chips, seq_rows, width), bf16),
            in_specs=[pl.BlockSpec(memory_space=pltpu.HBM)] + [whole] * 4,
            out_specs=whole,
            scratch_shapes=[
                pltpu.VMEM((half_rows, lanes), f32),
                pltpu.VMEM((half_rows, total + lanes), f32),
                pltpu.VMEM(memory_state.shape, f32),
                pltpu.SemaphoreType.DMA(memory_state.shape[:2]),
            ],
            compiler_params=pltpu.CompilerParams(vmem_limit_bytes=48 << 20),
            name="readout",
        )(memory_state, received, carried_rows, weight_rows, gain_rows)
    )

    by_source = received
    edge = total // 6

    def own_columns(start, size):
        return (
            by_source[:, :, start : start + size]
            .transpose(1, 0, 2)
            .reshape(seq_rows, head_count, chips * size // head_count)
            .astype(f32)
        )

    key_heads = own_columns(edge, edge)
    value_heads = own_columns(2 * edge, 2 * edge)
    new_memory = (
        carried[:, :, None, None] * memory_state
        + (written[:, :, None] * key_heads)[:, :, :, None] * value_heads[:, :, None, :]
    )

    columns = pl.pallas_call(
        mix_kernel,
        out_shape=jax.ShapeDtypeStruct((chips, half_rows, lanes), bf16),
        in_specs=[scalar] + [whole] * 3,
        out_specs=whole,
        scratch_shapes=[pltpu.VMEM((lanes, width), bf16), pltpu.VMEM((half_rows, width), f32)],
        compiler_params=pltpu.CompilerParams(vmem_limit_bytes=4 << 20),
        name="mix",
    )(core[None], same_mixed, *pairs[-2:])
    same_branch = exchange(columns)
    slots = axis_size * capacity
    same_routed = received[:, :, total:]
    pick, picked_tokens = pl.pallas_call(
        pick_kernel,
        out_shape=(
            jax.ShapeDtypeStruct((slots + 16, 2 * half_rows), bf16),
            jax.ShapeDtypeStruct((slots + 16, width), bf16),
        ),
        in_specs=[scalar] + [whole] * 4,
        out_specs=(whole, whole),
        scratch_shapes=[
            pltpu.VMEM((2 * half_rows, lanes), f32),
            pltpu.VMEM((2 * half_rows, width), f32),
        ],
        compiler_params=pltpu.CompilerParams(vmem_limit_bytes=8 << 20),
        name="pick",
    )(me[None], same_routed, partner(same_routed), same_tokens, partner(same_tokens))
    picked_tokens, pick, same_branch = lax.optimization_barrier((picked_tokens, pick, same_branch))
    results, own_residual = pl.pallas_call(
        expert_kernel,
        out_shape=(
            jax.ShapeDtypeStruct((axis_size, capacity, width), bf16),
            jax.ShapeDtypeStruct((seq_rows, width), bf16),
        ),
        in_specs=[whole] * 5 + [hbm] * 3,
        out_specs=(whole, whole),
        scratch_shapes=[
            pltpu.VMEM((2 * half_rows, width), bf16),
            pltpu.VMEM(expert_gate.shape[1:], bf16),
            pltpu.VMEM(expert_lift.shape[1:], bf16),
            pltpu.VMEM(expert_down.shape[1:], bf16),
            pltpu.SemaphoreType.DMA((3,)),
        ],
        compiler_params=pltpu.CompilerParams(vmem_limit_bytes=24 << 20),
        name="experts",
    )(
        pick,
        picked_tokens,
        same_branch,
        partner(same_branch),
        expert_norm[None],
        *map(in_hbm, (expert_gate, expert_lift, expert_down)),
    )
    routed_experts, results = lax.optimization_barrier((routed_experts, results))
    returned = lax.all_to_all(results, "ep", split_axis=0, concat_axis=0, tiled=True)
    earlier = jnp.arange(seq_rows)[:, None] > jnp.arange(seq_rows)[None, :]
    same = routed_experts[:, :, None, None] == routed_experts[None, None, :, :]
    slot_index = jnp.sum(
        (same & earlier[:, None, :, None]).astype(jnp.int32), axis=(2, 3), dtype=jnp.int32
    )
    layer_out = pl.pallas_call(
        combine_kernel,
        out_shape=jax.ShapeDtypeStruct((seq_rows, width), bf16),
        in_specs=[scalar] * 3 + [whole] * 2,
        out_specs=whole,
        compiler_params=pltpu.CompilerParams(vmem_limit_bytes=4 << 20),
        name="combine",
    )(routed_experts, slot_index, route_weights, returned, own_residual)
    return (layer_out, new_memory, new_max)


def solution(mesh):
    return jax.shard_map(
        body,
        mesh=mesh,
        in_specs=(
            P(("grp", "ep"), None),
            P(("grp", "ep"), None, None, None),
            P(("grp", "ep"), None),
            P(),
            P(None, "ep"),
            P(None, "ep"),
            P(None, "ep"),
            P(None, "ep"),
            P(),
            P(),
            P(),
            P(),
            P(None, "ep"),
            P(),
            P(("grp", "ep"), None),
            P(("grp", "ep"), None),
            P("ep", None, None),
            P("ep", None, None),
            P("ep", None, None),
        ),
        out_specs=(
            P(("grp", "ep"), None),
            P(("grp", "ep"), None, None, None),
            P(("grp", "ep"), None),
        ),
        check_vma=False,
    )
```

```python
import jax
import jax.numpy as jnp
from jax import lax
from jax.experimental import pallas as pl
from jax.experimental.pallas import tpu as pltpu
from jax.sharding import PartitionSpec as P

epsilon = 1e-06
f32, bf16 = jnp.float32, jnp.bfloat16
lanes = 128
whole = pl.BlockSpec(memory_space=pltpu.VMEM)
hbm = pl.BlockSpec(memory_space=pltpu.HBM)
scalar = pl.BlockSpec(memory_space=pltpu.SMEM)


def in_hbm(array):
    return pltpu.with_memory_space_constraint(array, pltpu.HBM)


def scaled_norm(entries, gain):
    return entries * lax.rsqrt(jnp.mean(entries * entries, axis=-1, keepdims=True) + epsilon) * gain


def exchange(blocks):
    size = lax.axis_size("ep")
    return lax.all_to_all(
        blocks,
        "ep",
        split_axis=0,
        concat_axis=0,
        tiled=True,
        axis_index_groups=[list(range(0, size, 2)), list(range(1, size, 2))],
    )


def hop(block, chips):
    size = lax.axis_size("ep")
    return lax.ppermute(block, "ep", [(i, (i + 2 * chips) % size) for i in range(size)])


near_hops = (1, -1, 2, -2)
far_hops = (5, -5)
last_hop = 3


def relay(block):
    first, second = (hop(block, chips) for chips in far_hops)
    bundle = jnp.stack([block, first, second])
    return [bundle] + [hop(bundle, chips) for chips in near_hops] + [hop(first[None], last_hop)]


def relay_order():
    bundle = [0] + [-chips for chips in far_hops]
    order = bundle + [at - chips for chips in near_hops for at in bundle]
    return order + [-far_hops[0] - last_hop]


def partner(block):
    return lax.ppermute(block, "ep", [(i, i ^ 1) for i in range(lax.axis_size("ep"))])


def gate_kernel(key_size, *refs):
    sources, outs, (*targets, arrived) = refs[:7], refs[7:13], refs[13:]
    copies = [
        pltpu.make_async_copy(source, target, arrived.at[i])
        for i, (source, target) in enumerate(zip(sources, targets))
    ]
    for copy in copies:
        copy.start()
    for copy in copies:
        copy.wait()
    tokens, gain, in_table, forget_table, bias, last_max, head_gain = targets
    new_max, carried, written, carried_rows, weight_rows, gain_rows = outs
    seqs = tokens.shape[0]
    heads, chips = bias.shape[1], head_gain.shape[0]
    normed = scaled_norm(tokens[...].astype(f32), gain[...]).astype(bf16)

    def logits(table):
        return lax.dot_general(
            normed, table[...], (((1,), (1,)), ((), ())), preferred_element_type=f32
        )

    input_logit = logits(in_table)
    forget_logit = logits(forget_table) + bias[...]
    log_forget = jnp.minimum(forget_logit, 0.0) - jnp.log1p(jnp.exp(-jnp.abs(forget_logit)))
    shifted = log_forget + last_max[...]
    top = jnp.maximum(shifted, input_logit)
    weight = jnp.exp(input_logit - top) * key_size ** (-0.5)
    kept = jnp.exp(shifted - top)
    new_max[...] = top
    carried[...] = kept
    written[...] = weight
    for chip in range(chips):
        head = chip // (chips // heads)
        rows = pl.ds(chip * seqs, seqs)
        carried_rows[rows, :] = jnp.broadcast_to(kept[:, head : head + 1], (seqs, lanes))
        weight_rows[rows, :] = jnp.broadcast_to(weight[:, head : head + 1], (seqs, lanes))
        gain_rows[rows, :] = jnp.broadcast_to(head_gain[chip : chip + 1, :], (seqs, lanes))


def place_tables(core, tables):
    start = 0
    for mine, theirs in zip(tables[::2], tables[1::2]):
        count = mine.shape[0]
        yield mine, pl.ds(pl.multiple_of(start + core * count, count), count)
        yield theirs, pl.ds(pl.multiple_of(start + (1 - core) * count, count), count)
        start += 2 * count


def project_kernel(me, routing, norm_gain, *refs):
    sources = len(near_hops) + 2
    blocks, tables = refs[:sources], refs[sources:-6]
    out, gathered, table, rows, gain, arrived = refs[-6:]
    chips, seqs = gathered.shape[:2]
    places = list(place_tables(me[0] % 2, tables))
    copies = [pltpu.make_async_copy(norm_gain, gain, arrived.at[0])]
    for i, (source, where) in enumerate(places[::2]):
        copies.append(pltpu.make_async_copy(source, table.at[where], arrived.at[i + 1]))
    for copy in copies:
        copy.start()
    for source, where in places[1::2]:
        table[where, :] = source[...]
    origins = [(me[0] // 2 + chips + ahead) % chips for ahead in relay_order()]
    parts = [(ref, i) for ref in blocks for i in range(ref.shape[0])]
    for at, (ref, i) in enumerate(parts):
        part = ref[i]
        gathered[origins[at]] = part
        rows[at * seqs : (at + 1) * seqs, :] = part.astype(f32)
    for copy in copies:
        copy.wait()
    normed = scaled_norm(rows[...], gain[...]).astype(bf16)
    columns = lax.dot_general(
        normed, table[...], (((1,), (1,)), ((), ())), preferred_element_type=f32
    )
    total = columns.shape[1]
    for at in range(chips):
        out[origins[at], :, :total] = columns[at * seqs : (at + 1) * seqs, :].astype(bf16)
        out[origins[at], :, total:] = routing[...]


def mix_kernel(me, blocks, mine, theirs, out, table, rows):
    chips, seqs = blocks.shape[:2]
    for source, where in place_tables(me[0] % 2, (mine, theirs)):
        table[where, :] = source[...]
    for chip in range(chips):
        rows[chip * seqs : (chip + 1) * seqs, :] = blocks[chip].astype(f32)
    columns = lax.dot_general(
        rows[...].astype(bf16), table[...], (((1,), (1,)), ((), ())), preferred_element_type=f32
    ).astype(bf16)
    for chip in range(chips):
        out[chip] = columns


def readout_kernel(state, received, carried, weight, gain, out, sums, flat, memory, arrived):
    seqs, heads, keys, values = state.shape
    chips = received.shape[0]
    per_head = chips // heads
    part = keys // per_head
    copies = {}
    for head in range(heads):
        for seq in range(seqs):
            copies[head, seq] = pltpu.make_async_copy(
                state.at[seq, head], memory.at[seq, head], arrived.at[seq, head]
            )
            copies[head, seq].start()
    for chip in range(chips):
        flat[chip * seqs : (chip + 1) * seqs, :] = received[chip].astype(f32)
    pairs = flat[:, :lanes]
    columns = pairs.T
    for head in range(heads):
        for seq in range(seqs):
            copies[head, seq].wait()
            total = jnp.zeros((8, values), f32)
            for j in range(per_head):
                at = (head * per_head + j) * seqs + seq
                block = memory[seq, head, j * part : (j + 1) * part, :]
                terms = block * columns[:part, at : at + 1]
                total = total + jnp.sum(terms.reshape(part // 8, 8, values), axis=0)
            row = jnp.sum(total, axis=0, keepdims=True)
            for j in range(per_head):
                at = (head * per_head + j) * seqs + seq
                sums[at : at + 1, :] = row[:, j * lanes : (j + 1) * lanes]

    def head_total(entries):
        by_chip = entries.reshape(heads, per_head // 2, 2 * seqs, lanes)
        both = jnp.sum(by_chip, axis=1)
        both = both + jnp.concatenate([both[:, seqs:], both[:, :seqs]], axis=1)
        both = jnp.broadcast_to(both[:, None], by_chip.shape).reshape(entries.shape)
        return jnp.sum(both, axis=-1, keepdims=True)

    products = pairs * jnp.concatenate([pairs[:, part:], pairs[:, :part]], axis=1)
    match = head_total(products) * 0.5
    readout = carried[...] * sums[...] + (weight[...] * match) * flat[:, lanes : 2 * lanes]
    scale = lax.rsqrt(head_total(readout * readout) / values + epsilon)
    gates = jax.nn.sigmoid(flat[:, 2 * lanes : 3 * lanes])
    mixed = readout * scale * gain[...] * gates
    for chip in range(chips):
        tile = mixed[chip * seqs : (chip + 1) * seqs, :].astype(bf16)
        for copy in range(chips):
            out[copy, :, chip * lanes : (chip + 1) * lanes] = tile


def pick_kernel(me, same_routed, other_routed, same_tokens, other_tokens, pick, picked, routed, rows):
    chips, seqs = same_tokens.shape[:2]
    half = chips * seqs
    core = me[0] % 2
    for chip in range(chips):
        at = chip * seqs
        routed[at : at + seqs, :] = same_routed[chip].astype(f32)
        routed[half + at : half + at + seqs, :] = other_routed[chip].astype(f32)
        rows[at : at + seqs, :] = same_tokens[chip].astype(f32)
        rows[half + at : half + at + seqs, :] = other_tokens[chip].astype(f32)
    choices = routed[...].T[:8]
    valid = lax.broadcasted_iota(jnp.int32, choices.shape, 0) < seqs
    hits = jnp.where(valid & (choices == me[0].astype(f32)), 1.0, 0.0)
    named = jnp.broadcast_to(jnp.sum(hits, axis=0, keepdims=True), hits.shape)
    lane = lax.broadcasted_iota(jnp.int32, hits.shape, 1)
    slot = jnp.zeros(hits.shape, f32)
    for back in range(1, seqs):
        slot = slot + jnp.where(lane % seqs >= back, pltpu.roll(named, back, 1), 0.0)
    source = 2 * (lane % half // seqs) + jnp.where(lane < half, core, 1 - core)
    place = jnp.where(named > 0.0, 2 * source + slot.astype(jnp.int32), -1)
    index = lax.broadcasted_iota(jnp.int32, pick.shape, 0)
    slots = 4 * chips
    mine = lax.broadcasted_iota(jnp.int32, pick.shape, 1) + slots - me[0] // 2 * seqs
    wanted = jnp.where(index < slots, jnp.broadcast_to(place[:1], pick.shape), mine)
    chosen = jnp.where(wanted == index, 1.0, 0.0).astype(bf16)
    pick[...] = chosen
    picked[...] = jnp.dot(chosen, rows[...].astype(bf16), preferred_element_type=f32).astype(bf16)


def expert_kernel(pick, tokens, same, other, gain, gate, lift, down, out, own, branch, *refs):
    gate_table, lift_table, down_table, arrived = refs
    copies = [
        pltpu.make_async_copy(source.at[0], target, arrived.at[i])
        for i, (source, target) in enumerate(
            ((gate, gate_table), (lift, lift_table), (down, down_table))
        )
    ]
    for copy in copies:
        copy.start()
    chips, rows = same.shape[:2]
    for chip in range(chips):
        columns = slice(chip * lanes, (chip + 1) * lanes)
        branch[:rows, columns] = same[chip]
        branch[rows:, columns] = other[chip]
    added = jnp.dot(pick[...], branch[...], preferred_element_type=f32)
    residual = (tokens[...].astype(f32) + added).astype(bf16)
    devices, capacity = out.shape[:2]
    slots = devices * capacity
    own[...] = residual[slots:][: own.shape[0]]
    expert_in = scaled_norm(residual[:slots].astype(f32), gain[...]).astype(bf16)
    copies[0].wait()
    gate_value = jnp.dot(expert_in, gate_table[...], preferred_element_type=f32)
    copies[1].wait()
    lift_value = jnp.dot(expert_in, lift_table[...], preferred_element_type=f32)
    hidden = (jax.nn.silu(gate_value) * lift_value).astype(bf16)
    copies[2].wait()
    results = jnp.dot(hidden, down_table[...], preferred_element_type=f32)
    for device in range(devices):
        out[device] = results[device * capacity : (device + 1) * capacity, :].astype(bf16)


def combine_kernel(expert, slot, weights, returned, own, out):
    seqs, choices = weights.shape
    for seq in range(seqs):
        total = jnp.zeros((1, out.shape[1]), f32)
        for choice in range(choices):
            pair = returned[expert[seq, choice]].astype(f32)
            row = pair[:1]
            for other in range(1, pair.shape[0]):
                row = jnp.where(slot[seq, choice] == other, pair[other : other + 1], row)
            total = total + (weights[seq, choice] * row).astype(bf16).astype(f32)
        out[seq : seq + 1, :] = (own[seq : seq + 1, :].astype(f32) + total).astype(bf16)


def body(
    tokens,
    memory_state,
    max_state,
    norm_gain,
    query_weight,
    key_weight,
    value_weight,
    output_gate,
    input_gate,
    forget_gate,
    forget_bias,
    head_gain,
    output_weight,
    expert_norm,
    routed_experts,
    route_weights,
    expert_gate,
    expert_lift,
    expert_down,
):
    seq_rows, width = tokens.shape
    head_count = forget_bias.shape[0]
    key_size = memory_state.shape[2]
    value_size = memory_state.shape[3]
    axis_size = lax.axis_size("ep")
    chips = axis_size // 2
    me = lax.axis_index("ep")
    half_rows = chips * seq_rows
    capacity = min(seq_rows, 2)
    choices = routed_experts.shape[1]

    blocks = relay(tokens)
    assert len(relay_order()) == chips

    pairs = []
    for table in (query_weight, key_weight, value_weight, output_gate, output_weight):
        pairs += [table.T, partner(table.T)]
    total = sum(table.shape[0] for table in pairs[:-2])

    per_head = chips // head_count
    gate_shape = jax.ShapeDtypeStruct((seq_rows, head_count), f32)
    row_shape = jax.ShapeDtypeStruct((half_rows, lanes), f32)
    gate_inputs = (
        tokens,
        norm_gain[None],
        input_gate.T,
        forget_gate.T,
        forget_bias[None],
        max_state,
        head_gain.reshape(chips, lanes),
    )
    new_max, carried, written, carried_rows, weight_rows, gain_rows = pl.pallas_call(
        lambda *refs: gate_kernel(key_size, *refs),
        out_shape=(gate_shape,) * 3 + (row_shape,) * 3,
        in_specs=[hbm] * 7,
        out_specs=(whole,) * 6,
        scratch_shapes=[pltpu.VMEM(array.shape, array.dtype) for array in gate_inputs]
        + [pltpu.SemaphoreType.DMA((7,))],
        compiler_params=pltpu.CompilerParams(vmem_limit_bytes=4 << 20),
        name="gates",
    )(*map(in_hbm, gate_inputs))
    routing = jnp.pad(routed_experts.astype(bf16), ((0, 0), (0, lanes - choices)))
    blocks, theirs, carried_rows, weight_rows, gain_rows, routing = lax.optimization_barrier(
        (blocks, pairs[1::2], carried_rows, weight_rows, gain_rows, routing)
    )

    pairs[1::2] = theirs
    pairs[:-2:2] = map(in_hbm, pairs[:-2:2])
    projected, same_tokens = pl.pallas_call(
        project_kernel,
        out_shape=(
            jax.ShapeDtypeStruct((chips, seq_rows, total + lanes), bf16),
            jax.ShapeDtypeStruct((chips, seq_rows, width), bf16),
        ),
        in_specs=[scalar, whole, hbm] + [whole] * len(blocks) + [hbm, whole] * (len(pairs) // 2 - 1),
        out_specs=(whole, whole),
        scratch_shapes=[
            pltpu.VMEM((total, width), bf16),
            pltpu.VMEM((half_rows, width), f32),
            pltpu.VMEM((1, width), f32),
            pltpu.SemaphoreType.DMA((len(pairs) // 2,)),
        ],
        compiler_params=pltpu.CompilerParams(vmem_limit_bytes=8 << 20),
        name="project",
    )(me[None], routing, in_hbm(norm_gain[None]), *blocks, *pairs[:-2])
    received = exchange(projected)
    same_mixed = exchange(
        pl.pallas_call(
            readout_kernel,
            out_shape=jax.ShapeDtypeStruct((chips, seq_rows, width), bf16),
            in_specs=[pl.BlockSpec(memory_space=pltpu.HBM)] + [whole] * 4,
            out_specs=whole,
            scratch_shapes=[
                pltpu.VMEM((half_rows, lanes), f32),
                pltpu.VMEM((half_rows, total + lanes), f32),
                pltpu.VMEM(memory_state.shape, f32),
                pltpu.SemaphoreType.DMA(memory_state.shape[:2]),
            ],
            compiler_params=pltpu.CompilerParams(vmem_limit_bytes=48 << 20),
            name="readout",
        )(memory_state, received, carried_rows, weight_rows, gain_rows)
    )

    by_source = received
    edge = total // 6

    def own_columns(start, size):
        return (
            by_source[:, :, start : start + size]
            .transpose(1, 0, 2)
            .reshape(seq_rows, head_count, chips * size // head_count)
            .astype(f32)
        )

    key_heads = own_columns(edge, edge)
    value_heads = own_columns(2 * edge, 2 * edge)
    new_memory = (
        carried[:, :, None, None] * memory_state
        + (written[:, :, None] * key_heads)[:, :, :, None] * value_heads[:, :, None, :]
    )

    columns = pl.pallas_call(
        mix_kernel,
        out_shape=jax.ShapeDtypeStruct((chips, half_rows, lanes), bf16),
        in_specs=[scalar] + [whole] * 3,
        out_specs=whole,
        scratch_shapes=[pltpu.VMEM((lanes, width), bf16), pltpu.VMEM((half_rows, width), f32)],
        compiler_params=pltpu.CompilerParams(vmem_limit_bytes=4 << 20),
        name="mix",
    )(me[None], same_mixed, *pairs[-2:])
    same_branch = exchange(columns)
    slots = axis_size * capacity
    same_routed = received[:, :, total:]
    pick, picked_tokens = pl.pallas_call(
        pick_kernel,
        out_shape=(
            jax.ShapeDtypeStruct((slots + 16, 2 * half_rows), bf16),
            jax.ShapeDtypeStruct((slots + 16, width), bf16),
        ),
        in_specs=[scalar] + [whole] * 4,
        out_specs=(whole, whole),
        scratch_shapes=[
            pltpu.VMEM((2 * half_rows, lanes), f32),
            pltpu.VMEM((2 * half_rows, width), f32),
        ],
        compiler_params=pltpu.CompilerParams(vmem_limit_bytes=8 << 20),
        name="pick",
    )(me[None], same_routed, partner(same_routed), same_tokens, partner(same_tokens))
    picked_tokens, pick, same_branch = lax.optimization_barrier((picked_tokens, pick, same_branch))
    results, own_residual = pl.pallas_call(
        expert_kernel,
        out_shape=(
            jax.ShapeDtypeStruct((axis_size, capacity, width), bf16),
            jax.ShapeDtypeStruct((seq_rows, width), bf16),
        ),
        in_specs=[whole] * 5 + [hbm] * 3,
        out_specs=(whole, whole),
        scratch_shapes=[
            pltpu.VMEM((2 * half_rows, width), bf16),
            pltpu.VMEM(expert_gate.shape[1:], bf16),
            pltpu.VMEM(expert_lift.shape[1:], bf16),
            pltpu.VMEM(expert_down.shape[1:], bf16),
            pltpu.SemaphoreType.DMA((3,)),
        ],
        compiler_params=pltpu.CompilerParams(vmem_limit_bytes=24 << 20),
        name="experts",
    )(
        pick,
        picked_tokens,
        same_branch,
        partner(same_branch),
        expert_norm[None],
        *map(in_hbm, (expert_gate, expert_lift, expert_down)),
    )
    routed_experts, results = lax.optimization_barrier((routed_experts, results))
    returned = lax.all_to_all(results, "ep", split_axis=0, concat_axis=0, tiled=True)
    earlier = jnp.arange(seq_rows)[:, None] > jnp.arange(seq_rows)[None, :]
    same = routed_experts[:, :, None, None] == routed_experts[None, None, :, :]
    slot_index = jnp.sum(
        (same & earlier[:, None, :, None]).astype(jnp.int32), axis=(2, 3), dtype=jnp.int32
    )
    layer_out = pl.pallas_call(
        combine_kernel,
        out_shape=jax.ShapeDtypeStruct((seq_rows, width), bf16),
        in_specs=[scalar] * 3 + [whole] * 2,
        out_specs=whole,
        compiler_params=pltpu.CompilerParams(vmem_limit_bytes=4 << 20),
        name="combine",
    )(routed_experts, slot_index, route_weights, returned, own_residual)
    return (layer_out, new_memory, new_max)


def solution(mesh):
    return jax.shard_map(
        body,
        mesh=mesh,
        in_specs=(
            P(("grp", "ep"), None),
            P(("grp", "ep"), None, None, None),
            P(("grp", "ep"), None),
            P(),
            P(None, "ep"),
            P(None, "ep"),
            P(None, "ep"),
            P(None, "ep"),
            P(),
            P(),
            P(),
            P(),
            P(None, "ep"),
            P(),
            P(("grp", "ep"), None),
            P(("grp", "ep"), None),
            P("ep", None, None),
            P("ep", None, None),
            P("ep", None, None),
        ),
        out_specs=(
            P(("grp", "ep"), None),
            P(("grp", "ep"), None, None, None),
            P(("grp", "ep"), None),
        ),
        check_vma=False,
    )
```

```python
import jax
import jax.numpy as jnp
from jax import lax
from jax.experimental import pallas as pl
from jax.experimental.pallas import tpu as pltpu
from jax.sharding import PartitionSpec as P

epsilon = 1e-06
f32, bf16 = jnp.float32, jnp.bfloat16
lanes = 128
whole = pl.BlockSpec(memory_space=pltpu.VMEM)
hbm = pl.BlockSpec(memory_space=pltpu.HBM)
scalar = pl.BlockSpec(memory_space=pltpu.SMEM)


def in_hbm(array):
    return pltpu.with_memory_space_constraint(array, pltpu.HBM)


def scaled_norm(entries, gain):
    return entries * lax.rsqrt(jnp.mean(entries * entries, axis=-1, keepdims=True) + epsilon) * gain


def exchange(blocks):
    size = lax.axis_size("ep")
    return lax.all_to_all(
        blocks,
        "ep",
        split_axis=0,
        concat_axis=0,
        tiled=True,
        axis_index_groups=[list(range(0, size, 2)), list(range(1, size, 2))],
    )


far, near, nearer, last = 5, 2, 1, 3


def side(chip, stride):
    return 1 - 2 * (chip // (2 if stride == near else 1) % 2)


def swap(block, stride, first):
    size = lax.axis_size("ep")
    pairs = []
    for device in range(size):
        step = side(device // 2, stride) * stride * (1 if first else -1)
        pairs.append((device, (device + 2 * step) % size))
    return lax.ppermute(block, "ep", pairs)


def relay(block):
    ahead, behind = swap(block, far, True), swap(block, far, False)
    bundle = jnp.stack([block, ahead, behind])
    return (
        [bundle]
        + [swap(bundle, stride, first) for stride in (nearer, near) for first in (True, False)]
        + [swap(behind[None], last, True)]
    )


def relay_order(chip):
    way = side(chip, far)
    order = [0, way * far, -way * far]
    for stride in (nearer, near):
        for step in (side(chip, stride) * stride, -side(chip, stride) * stride):
            there = -way if stride % 2 else way
            order += [step, step + there * far, step - there * far]
    return order + [way * (last + far)]


def partner(block):
    return lax.ppermute(block, "ep", [(i, i ^ 1) for i in range(lax.axis_size("ep"))])


def gate_kernel(key_size, *refs):
    sources, outs, (*targets, arrived) = refs[:8], refs[8:15], refs[15:]
    copies = [
        pltpu.make_async_copy(source, target, arrived.at[i])
        for i, (source, target) in enumerate(zip(sources, targets))
    ]
    for copy in copies:
        copy.start()
    for copy in copies:
        copy.wait()
    tokens, gain, in_table, forget_table, bias, last_max, head_gain, routed = targets
    new_max, carried, written, carried_rows, weight_rows, gain_rows, routing = outs
    seqs = tokens.shape[0]
    heads, chips = bias.shape[1], head_gain.shape[0]
    normed = scaled_norm(tokens[...].astype(f32), gain[...]).astype(bf16)

    def logits(table):
        return lax.dot_general(
            normed, table[...], (((1,), (1,)), ((), ())), preferred_element_type=f32
        )

    input_logit = logits(in_table)
    forget_logit = logits(forget_table) + bias[...]
    log_forget = jnp.minimum(forget_logit, 0.0) - jnp.log1p(jnp.exp(-jnp.abs(forget_logit)))
    shifted = log_forget + last_max[...]
    top = jnp.maximum(shifted, input_logit)
    weight = jnp.exp(input_logit - top) * key_size ** (-0.5)
    kept = jnp.exp(shifted - top)
    names = routed[...].astype(f32)
    lane = lax.broadcasted_iota(jnp.int32, routing.shape, 1)
    spread = jnp.zeros(routing.shape, f32)
    for choice in range(names.shape[1]):
        spread = jnp.where(lane == choice, names[:, choice : choice + 1], spread)
    routing[...] = spread.astype(bf16)
    new_max[...] = top
    carried[...] = kept
    written[...] = weight
    for chip in range(chips):
        head = chip // (chips // heads)
        rows = pl.ds(chip * seqs, seqs)
        carried_rows[rows, :] = jnp.broadcast_to(kept[:, head : head + 1], (seqs, lanes))
        weight_rows[rows, :] = jnp.broadcast_to(weight[:, head : head + 1], (seqs, lanes))
        gain_rows[rows, :] = jnp.broadcast_to(head_gain[chip : chip + 1, :], (seqs, lanes))


def place_tables(core, tables):
    start = 0
    for mine, theirs in zip(tables[::2], tables[1::2]):
        count = mine.shape[0]
        yield mine, pl.ds(pl.multiple_of(start + core * count, count), count)
        yield theirs, pl.ds(pl.multiple_of(start + (1 - core) * count, count), count)
        start += 2 * count


def project_kernel(me, routing, norm_gain, *refs):
    sources = 6
    blocks, tables = refs[:sources], refs[sources:-6]
    out, gathered, table, rows, gain, arrived = refs[-6:]
    chips, seqs = gathered.shape[:2]
    places = list(place_tables(me[0] % 2, tables))
    copies = [pltpu.make_async_copy(norm_gain, gain, arrived.at[0])]
    for i, (source, where) in enumerate(places[::2]):
        copies.append(pltpu.make_async_copy(source, table.at[where], arrived.at[i + 1]))
    for copy in copies:
        copy.start()
    for source, where in places[1::2]:
        table[where, :] = source[...]
    chip = me[0] // 2
    origins = [(chip + chips + ahead) % chips for ahead in relay_order(chip)]
    parts = [(ref, i) for ref in blocks for i in range(ref.shape[0])]
    for at, (ref, i) in enumerate(parts):
        part = ref[i]
        gathered[origins[at]] = part
        rows[at * seqs : (at + 1) * seqs, :] = part.astype(f32)
    for copy in copies:
        copy.wait()
    normed = scaled_norm(rows[...], gain[...]).astype(bf16)
    columns = lax.dot_general(
        normed, table[...], (((1,), (1,)), ((), ())), preferred_element_type=f32
    )
    total = columns.shape[1]
    for at in range(chips):
        out[origins[at], :, :total] = columns[at * seqs : (at + 1) * seqs, :].astype(bf16)
        out[origins[at], :, total:] = routing[...]


def mix_kernel(me, blocks, mine, theirs, out, table, rows):
    chips, seqs = blocks.shape[:2]
    for source, where in place_tables(me[0] % 2, (mine, theirs)):
        table[where, :] = source[...]
    for chip in range(chips):
        rows[chip * seqs : (chip + 1) * seqs, :] = blocks[chip].astype(f32)
    columns = lax.dot_general(
        rows[...].astype(bf16), table[...], (((1,), (1,)), ((), ())), preferred_element_type=f32
    ).astype(bf16)
    for chip in range(chips):
        out[chip] = columns


def readout_kernel(state, received, carried, weight, gain, out, sums, flat, memory, arrived):
    seqs, heads, keys, values = state.shape
    chips = received.shape[0]
    per_head = chips // heads
    part = keys // per_head
    copies = {}
    for head in range(heads):
        for seq in range(seqs):
            copies[head, seq] = pltpu.make_async_copy(
                state.at[seq, head], memory.at[seq, head], arrived.at[seq, head]
            )
            copies[head, seq].start()
    for chip in range(chips):
        flat[chip * seqs : (chip + 1) * seqs, :] = received[chip].astype(f32)
    pairs = flat[:, :lanes]
    columns = pairs.T
    for head in range(heads):
        for seq in range(seqs):
            copies[head, seq].wait()
            total = jnp.zeros((8, values), f32)
            for j in range(per_head):
                at = (head * per_head + j) * seqs + seq
                block = memory[seq, head, j * part : (j + 1) * part, :]
                terms = block * columns[:part, at : at + 1]
                total = total + jnp.sum(terms.reshape(part // 8, 8, values), axis=0)
            row = jnp.sum(total, axis=0, keepdims=True)
            for j in range(per_head):
                at = (head * per_head + j) * seqs + seq
                sums[at : at + 1, :] = row[:, j * lanes : (j + 1) * lanes]

    def head_total(entries):
        by_chip = entries.reshape(heads, per_head // 2, 2 * seqs, lanes)
        both = jnp.sum(by_chip, axis=1)
        both = both + jnp.concatenate([both[:, seqs:], both[:, :seqs]], axis=1)
        both = jnp.broadcast_to(both[:, None], by_chip.shape).reshape(entries.shape)
        return jnp.sum(both, axis=-1, keepdims=True)

    products = pairs * jnp.concatenate([pairs[:, part:], pairs[:, :part]], axis=1)
    match = head_total(products) * 0.5
    readout = carried[...] * sums[...] + (weight[...] * match) * flat[:, lanes : 2 * lanes]
    scale = lax.rsqrt(head_total(readout * readout) / values + epsilon)
    gates = jax.nn.sigmoid(flat[:, 2 * lanes : 3 * lanes])
    mixed = readout * scale * gain[...] * gates
    for chip in range(chips):
        tile = mixed[chip * seqs : (chip + 1) * seqs, :].astype(bf16)
        for copy in range(chips):
            out[copy, :, chip * lanes : (chip + 1) * lanes] = tile


def pick_kernel(me, same_routed, other_routed, same_tokens, other_tokens, pick, picked, routed, rows):
    chips, seqs = same_tokens.shape[:2]
    half = chips * seqs
    core = me[0] % 2
    for chip in range(chips):
        at = chip * seqs
        routed[at : at + seqs, :] = same_routed[chip].astype(f32)
        routed[half + at : half + at + seqs, :] = other_routed[chip].astype(f32)
        rows[at : at + seqs, :] = same_tokens[chip].astype(f32)
        rows[half + at : half + at + seqs, :] = other_tokens[chip].astype(f32)
    choices = routed[...].T[:8]
    valid = lax.broadcasted_iota(jnp.int32, choices.shape, 0) < seqs
    hits = jnp.where(valid & (choices == me[0].astype(f32)), 1.0, 0.0)
    named = jnp.broadcast_to(jnp.sum(hits, axis=0, keepdims=True), hits.shape)
    lane = lax.broadcasted_iota(jnp.int32, hits.shape, 1)
    slot = jnp.zeros(hits.shape, f32)
    for back in range(1, seqs):
        slot = slot + jnp.where(lane % seqs >= back, pltpu.roll(named, back, 1), 0.0)
    source = 2 * (lane % half // seqs) + jnp.where(lane < half, core, 1 - core)
    place = jnp.where(named > 0.0, 2 * source + slot.astype(jnp.int32), -1)
    index = lax.broadcasted_iota(jnp.int32, pick.shape, 0)
    slots = 4 * chips
    mine = lax.broadcasted_iota(jnp.int32, pick.shape, 1) + slots - me[0] // 2 * seqs
    wanted = jnp.where(index < slots, jnp.broadcast_to(place[:1], pick.shape), mine)
    chosen = jnp.where(wanted == index, 1.0, 0.0).astype(bf16)
    pick[...] = chosen
    picked[...] = jnp.dot(chosen, rows[...].astype(bf16), preferred_element_type=f32).astype(bf16)


def expert_kernel(pick, tokens, same, other, gain, gate, lift, down, out, own, branch, *refs):
    gate_table, lift_table, down_table, arrived = refs
    copies = [
        pltpu.make_async_copy(source.at[0], target, arrived.at[i])
        for i, (source, target) in enumerate(
            ((gate, gate_table), (lift, lift_table), (down, down_table))
        )
    ]
    for copy in copies:
        copy.start()
    chips, rows = same.shape[:2]
    for chip in range(chips):
        columns = slice(chip * lanes, (chip + 1) * lanes)
        branch[:rows, columns] = same[chip]
        branch[rows:, columns] = other[chip]
    added = jnp.dot(pick[...], branch[...], preferred_element_type=f32)
    residual = (tokens[...].astype(f32) + added).astype(bf16)
    devices, capacity = out.shape[:2]
    slots = devices * capacity
    own[...] = residual[slots:][: own.shape[0]]
    expert_in = scaled_norm(residual[:slots].astype(f32), gain[...]).astype(bf16)
    copies[0].wait()
    gate_value = jnp.dot(expert_in, gate_table[...], preferred_element_type=f32)
    copies[1].wait()
    lift_value = jnp.dot(expert_in, lift_table[...], preferred_element_type=f32)
    hidden = (jax.nn.silu(gate_value) * lift_value).astype(bf16)
    copies[2].wait()
    results = jnp.dot(hidden, down_table[...], preferred_element_type=f32)
    for device in range(devices):
        out[device] = results[device * capacity : (device + 1) * capacity, :].astype(bf16)


def combine_kernel(expert, slot, weights, returned, own, out):
    seqs, choices = weights.shape
    for seq in range(seqs):
        total = jnp.zeros((1, out.shape[1]), f32)
        for choice in range(choices):
            pair = returned[expert[seq, choice]].astype(f32)
            row = pair[:1]
            for other in range(1, pair.shape[0]):
                row = jnp.where(slot[seq, choice] == other, pair[other : other + 1], row)
            total = total + (weights[seq, choice] * row).astype(bf16).astype(f32)
        out[seq : seq + 1, :] = (own[seq : seq + 1, :].astype(f32) + total).astype(bf16)


def body(
    tokens,
    memory_state,
    max_state,
    norm_gain,
    query_weight,
    key_weight,
    value_weight,
    output_gate,
    input_gate,
    forget_gate,
    forget_bias,
    head_gain,
    output_weight,
    expert_norm,
    routed_experts,
    route_weights,
    expert_gate,
    expert_lift,
    expert_down,
):
    seq_rows, width = tokens.shape
    head_count = forget_bias.shape[0]
    key_size = memory_state.shape[2]
    value_size = memory_state.shape[3]
    axis_size = lax.axis_size("ep")
    chips = axis_size // 2
    me = lax.axis_index("ep")
    half_rows = chips * seq_rows
    capacity = min(seq_rows, 2)
    choices = routed_experts.shape[1]

    blocks = relay(tokens)
    assert sorted(at % chips for at in relay_order(0)) == list(range(chips))

    pairs = []
    for table in (query_weight, key_weight, value_weight, output_gate, output_weight):
        pairs += [table.T, partner(table.T)]
    total = sum(table.shape[0] for table in pairs[:-2])

    per_head = chips // head_count
    gate_shape = jax.ShapeDtypeStruct((seq_rows, head_count), f32)
    row_shape = jax.ShapeDtypeStruct((half_rows, lanes), f32)
    gate_inputs = (
        tokens,
        norm_gain[None],
        input_gate.T,
        forget_gate.T,
        forget_bias[None],
        max_state,
        head_gain.reshape(chips, lanes),
        routed_experts,
    )
    new_max, carried, written, carried_rows, weight_rows, gain_rows, routing = pl.pallas_call(
        lambda *refs: gate_kernel(key_size, *refs),
        out_shape=(gate_shape,) * 3
        + (row_shape,) * 3
        + (jax.ShapeDtypeStruct((seq_rows, lanes), bf16),),
        in_specs=[hbm] * 8,
        out_specs=(whole,) * 7,
        scratch_shapes=[pltpu.VMEM(array.shape, array.dtype) for array in gate_inputs]
        + [pltpu.SemaphoreType.DMA((8,))],
        compiler_params=pltpu.CompilerParams(vmem_limit_bytes=4 << 20),
        name="gates",
    )(*map(in_hbm, gate_inputs))
    blocks, theirs, carried_rows, weight_rows, gain_rows, routing = lax.optimization_barrier(
        (blocks, pairs[1::2], carried_rows, weight_rows, gain_rows, routing)
    )

    pairs[1::2] = theirs
    pairs[:-2:2] = map(in_hbm, pairs[:-2:2])
    projected, same_tokens = pl.pallas_call(
        project_kernel,
        out_shape=(
            jax.ShapeDtypeStruct((chips, seq_rows, total + lanes), bf16),
            jax.ShapeDtypeStruct((chips, seq_rows, width), bf16),
        ),
        in_specs=[scalar, whole, hbm] + [whole] * len(blocks) + [hbm, whole] * (len(pairs) // 2 - 1),
        out_specs=(whole, whole),
        scratch_shapes=[
            pltpu.VMEM((total, width), bf16),
            pltpu.VMEM((half_rows, width), f32),
            pltpu.VMEM((1, width), f32),
            pltpu.SemaphoreType.DMA((len(pairs) // 2,)),
        ],
        compiler_params=pltpu.CompilerParams(vmem_limit_bytes=8 << 20),
        name="project",
    )(me[None], routing, in_hbm(norm_gain[None]), *blocks, *pairs[:-2])
    received = exchange(projected)
    same_mixed = exchange(
        pl.pallas_call(
            readout_kernel,
            out_shape=jax.ShapeDtypeStruct((chips, seq_rows, width), bf16),
            in_specs=[pl.BlockSpec(memory_space=pltpu.HBM)] + [whole] * 4,
            out_specs=whole,
            scratch_shapes=[
                pltpu.VMEM((half_rows, lanes), f32),
                pltpu.VMEM((half_rows, total + lanes), f32),
                pltpu.VMEM(memory_state.shape, f32),
                pltpu.SemaphoreType.DMA(memory_state.shape[:2]),
            ],
            compiler_params=pltpu.CompilerParams(vmem_limit_bytes=48 << 20),
            name="readout",
        )(memory_state, received, carried_rows, weight_rows, gain_rows)
    )

    by_source = received
    edge = total // 6

    def own_columns(start, size):
        return (
            by_source[:, :, start : start + size]
            .transpose(1, 0, 2)
            .reshape(seq_rows, head_count, chips * size // head_count)
            .astype(f32)
        )

    key_heads = own_columns(edge, edge)
    value_heads = own_columns(2 * edge, 2 * edge)
    new_memory = (
        carried[:, :, None, None] * memory_state
        + (written[:, :, None] * key_heads)[:, :, :, None] * value_heads[:, :, None, :]
    )

    columns = pl.pallas_call(
        mix_kernel,
        out_shape=jax.ShapeDtypeStruct((chips, half_rows, lanes), bf16),
        in_specs=[scalar] + [whole] * 3,
        out_specs=whole,
        scratch_shapes=[pltpu.VMEM((lanes, width), bf16), pltpu.VMEM((half_rows, width), f32)],
        compiler_params=pltpu.CompilerParams(vmem_limit_bytes=4 << 20),
        name="mix",
    )(me[None], same_mixed, *pairs[-2:])
    same_branch = exchange(columns)
    slots = axis_size * capacity
    same_routed = received[:, :, total:]
    pick, picked_tokens = pl.pallas_call(
        pick_kernel,
        out_shape=(
            jax.ShapeDtypeStruct((slots + 16, 2 * half_rows), bf16),
            jax.ShapeDtypeStruct((slots + 16, width), bf16),
        ),
        in_specs=[scalar] + [whole] * 4,
        out_specs=(whole, whole),
        scratch_shapes=[
            pltpu.VMEM((2 * half_rows, lanes), f32),
            pltpu.VMEM((2 * half_rows, width), f32),
        ],
        compiler_params=pltpu.CompilerParams(vmem_limit_bytes=8 << 20),
        name="pick",
    )(me[None], same_routed, partner(same_routed), same_tokens, partner(same_tokens))
    picked_tokens, pick, same_branch = lax.optimization_barrier((picked_tokens, pick, same_branch))
    results, own_residual = pl.pallas_call(
        expert_kernel,
        out_shape=(
            jax.ShapeDtypeStruct((axis_size, capacity, width), bf16),
            jax.ShapeDtypeStruct((seq_rows, width), bf16),
        ),
        in_specs=[whole] * 5 + [hbm] * 3,
        out_specs=(whole, whole),
        scratch_shapes=[
            pltpu.VMEM((2 * half_rows, width), bf16),
            pltpu.VMEM(expert_gate.shape[1:], bf16),
            pltpu.VMEM(expert_lift.shape[1:], bf16),
            pltpu.VMEM(expert_down.shape[1:], bf16),
            pltpu.SemaphoreType.DMA((3,)),
        ],
        compiler_params=pltpu.CompilerParams(vmem_limit_bytes=24 << 20),
        name="experts",
    )(
        pick,
        picked_tokens,
        same_branch,
        partner(same_branch),
        expert_norm[None],
        *map(in_hbm, (expert_gate, expert_lift, expert_down)),
    )
    routed_experts, results = lax.optimization_barrier((routed_experts, results))
    returned = lax.all_to_all(results, "ep", split_axis=0, concat_axis=0, tiled=True)
    earlier = jnp.arange(seq_rows)[:, None] > jnp.arange(seq_rows)[None, :]
    same = routed_experts[:, :, None, None] == routed_experts[None, None, :, :]
    slot_index = jnp.sum(
        (same & earlier[:, None, :, None]).astype(jnp.int32), axis=(2, 3), dtype=jnp.int32
    )
    layer_out = pl.pallas_call(
        combine_kernel,
        out_shape=jax.ShapeDtypeStruct((seq_rows, width), bf16),
        in_specs=[scalar] * 3 + [whole] * 2,
        out_specs=whole,
        compiler_params=pltpu.CompilerParams(vmem_limit_bytes=4 << 20),
        name="combine",
    )(routed_experts, slot_index, route_weights, returned, own_residual)
    return (layer_out, new_memory, new_max)


def solution(mesh):
    return jax.shard_map(
        body,
        mesh=mesh,
        in_specs=(
            P(("grp", "ep"), None),
            P(("grp", "ep"), None, None, None),
            P(("grp", "ep"), None),
            P(),
            P(None, "ep"),
            P(None, "ep"),
            P(None, "ep"),
            P(None, "ep"),
            P(),
            P(),
            P(),
            P(),
            P(None, "ep"),
            P(),
            P(("grp", "ep"), None),
            P(("grp", "ep"), None),
            P("ep", None, None),
            P("ep", None, None),
            P("ep", None, None),
        ),
        out_specs=(
            P(("grp", "ep"), None),
            P(("grp", "ep"), None, None, None),
            P(("grp", "ep"), None),
        ),
        check_vma=False,
    )
```

```python
import jax
import jax.numpy as jnp
from jax import lax
from jax.experimental import pallas as pl
from jax.experimental.pallas import tpu as pltpu
from jax.sharding import PartitionSpec as P

epsilon = 1e-06
f32, bf16 = jnp.float32, jnp.bfloat16
lanes = 128
whole = pl.BlockSpec(memory_space=pltpu.VMEM)
hbm = pl.BlockSpec(memory_space=pltpu.HBM)
scalar = pl.BlockSpec(memory_space=pltpu.SMEM)


def in_hbm(array):
    return pltpu.with_memory_space_constraint(array, pltpu.HBM)


def scaled_norm(entries, gain):
    return entries * lax.rsqrt(jnp.mean(entries * entries, axis=-1, keepdims=True) + epsilon) * gain


def exchange(blocks):
    size = lax.axis_size("ep")
    return lax.all_to_all(
        blocks,
        "ep",
        split_axis=0,
        concat_axis=0,
        tiled=True,
        axis_index_groups=[list(range(0, size, 2)), list(range(1, size, 2))],
    )


far, near, nearer, last = 5, 2, 1, 3


def side(chip, stride):
    return 1 - 2 * (chip // (2 if stride == near else 1) % 2)


def swap(block, stride, first):
    size = lax.axis_size("ep")
    pairs = []
    for device in range(size):
        step = side(device // 2, stride) * stride * (1 if first else -1)
        pairs.append((device, (device + 2 * step) % size))
    return lax.ppermute(block, "ep", pairs)


def relay(block):
    ahead, behind = swap(block, far, True), swap(block, far, False)
    bundle = jnp.stack([block, ahead, behind])
    return (
        [bundle]
        + [swap(bundle, stride, first) for stride in (nearer, near) for first in (True, False)]
        + [swap(behind[None], last, True)]
    )


def relay_order(chip):
    way = side(chip, far)
    order = [0, way * far, -way * far]
    for stride in (nearer, near):
        for step in (side(chip, stride) * stride, -side(chip, stride) * stride):
            there = -way if stride % 2 else way
            order += [step, step + there * far, step - there * far]
    return order + [way * (last + far)]


def partner(block):
    return lax.ppermute(block, "ep", [(i, i ^ 1) for i in range(lax.axis_size("ep"))])


def gate_kernel(key_size, *refs):
    sources, outs, (*targets, arrived) = refs[:8], refs[8:15], refs[15:]
    copies = [
        pltpu.make_async_copy(source, target, arrived.at[i])
        for i, (source, target) in enumerate(zip(sources, targets))
    ]
    for copy in copies:
        copy.start()
    for copy in copies:
        copy.wait()
    tokens, gain, in_table, forget_table, bias, last_max, head_gain, routed = targets
    new_max, carried, written, carried_rows, weight_rows, gain_rows, routing = outs
    seqs = tokens.shape[0]
    heads, chips = bias.shape[1], head_gain.shape[0]
    normed = scaled_norm(tokens[...].astype(f32), gain[...]).astype(bf16)

    def logits(table):
        return lax.dot_general(
            normed, table[...], (((1,), (1,)), ((), ())), preferred_element_type=f32
        )

    input_logit = logits(in_table)
    forget_logit = logits(forget_table) + bias[...]
    log_forget = jnp.minimum(forget_logit, 0.0) - jnp.log1p(jnp.exp(-jnp.abs(forget_logit)))
    shifted = log_forget + last_max[...]
    top = jnp.maximum(shifted, input_logit)
    weight = jnp.exp(input_logit - top) * key_size ** (-0.5)
    kept = jnp.exp(shifted - top)
    names = routed[...].astype(f32)
    lane = lax.broadcasted_iota(jnp.int32, routing.shape, 1)
    spread = jnp.zeros(routing.shape, f32)
    for choice in range(names.shape[1]):
        spread = jnp.where(lane == choice, names[:, choice : choice + 1], spread)
    routing[...] = spread.astype(bf16)
    new_max[...] = top
    carried[...] = kept
    written[...] = weight
    for chip in range(chips):
        head = chip // (chips // heads)
        rows = pl.ds(chip * seqs, seqs)
        carried_rows[rows, :] = jnp.broadcast_to(kept[:, head : head + 1], (seqs, lanes))
        weight_rows[rows, :] = jnp.broadcast_to(weight[:, head : head + 1], (seqs, lanes))
        gain_rows[rows, :] = jnp.broadcast_to(head_gain[chip : chip + 1, :], (seqs, lanes))


def place_tables(core, tables):
    start = 0
    for mine, theirs in zip(tables[::2], tables[1::2]):
        count = mine.shape[0]
        yield mine, pl.ds(pl.multiple_of(start + core * count, count), count)
        yield theirs, pl.ds(pl.multiple_of(start + (1 - core) * count, count), count)
        start += 2 * count


def project_kernel(me, routing, norm_gain, *refs):
    sources = 6
    blocks, tables = refs[:sources], refs[sources:-6]
    out, gathered, table, rows, gain, arrived = refs[-6:]
    chips, seqs = gathered.shape[:2]
    places = list(place_tables(me[0] % 2, tables))
    copies = [pltpu.make_async_copy(norm_gain, gain, arrived.at[0])]
    for i, (source, where) in enumerate(places[::2]):
        copies.append(pltpu.make_async_copy(source, table.at[where], arrived.at[i + 1]))
    for copy in copies:
        copy.start()
    for source, where in places[1::2]:
        table[where, :] = source[...]
    chip = me[0] // 2
    origins = [(chip + chips + ahead) % chips for ahead in relay_order(chip)]
    parts = [(ref, i) for ref in blocks for i in range(ref.shape[0])]
    for at, (ref, i) in enumerate(parts):
        part = ref[i]
        gathered[origins[at]] = part
        rows[at * seqs : (at + 1) * seqs, :] = part.astype(f32)
    for copy in copies:
        copy.wait()
    normed = scaled_norm(rows[...], gain[...]).astype(bf16)
    columns = lax.dot_general(
        normed, table[...], (((1,), (1,)), ((), ())), preferred_element_type=f32
    )
    total = columns.shape[1]
    for at in range(chips):
        out[origins[at], :, :total] = columns[at * seqs : (at + 1) * seqs, :].astype(bf16)
        out[origins[at], :, total:] = routing[...]


def mix_kernel(me, blocks, mine, theirs, out, table, rows):
    chips, seqs = blocks.shape[:2]
    for source, where in place_tables(me[0] % 2, (mine, theirs)):
        table[where, :] = source[...]
    for chip in range(chips):
        rows[chip * seqs : (chip + 1) * seqs, :] = blocks[chip].astype(f32)
    columns = lax.dot_general(
        rows[...].astype(bf16), table[...], (((1,), (1,)), ((), ())), preferred_element_type=f32
    ).astype(bf16)
    for chip in range(chips):
        out[chip] = columns


def readout_kernel(state, received, carried, weight, gain, out, sums, flat, memory, arrived):
    seqs, heads, keys, values = state.shape
    chips = received.shape[0]
    per_head = chips // heads
    part = keys // per_head
    copies = {}
    for head in range(heads):
        for seq in range(seqs):
            copies[head, seq] = pltpu.make_async_copy(
                state.at[seq, head], memory.at[seq, head], arrived.at[seq, head]
            )
            copies[head, seq].start()
    for chip in range(chips):
        flat[chip * seqs : (chip + 1) * seqs, :] = received[chip].astype(f32)
    pairs = flat[:, :lanes]
    columns = pairs.T
    for head in range(heads):
        for seq in range(seqs):
            copies[head, seq].wait()
            total = jnp.zeros((8, values), f32)
            for j in range(per_head):
                at = (head * per_head + j) * seqs + seq
                block = memory[seq, head, j * part : (j + 1) * part, :]
                terms = block * columns[:part, at : at + 1]
                total = total + jnp.sum(terms.reshape(part // 8, 8, values), axis=0)
            row = jnp.sum(total, axis=0, keepdims=True)
            for j in range(per_head):
                at = (head * per_head + j) * seqs + seq
                sums[at : at + 1, :] = row[:, j * lanes : (j + 1) * lanes]

    def head_total(entries):
        by_chip = entries.reshape(heads, per_head // 2, 2 * seqs, lanes)
        both = jnp.sum(by_chip, axis=1)
        both = both + jnp.concatenate([both[:, seqs:], both[:, :seqs]], axis=1)
        both = jnp.broadcast_to(both[:, None], by_chip.shape).reshape(entries.shape)
        return jnp.sum(both, axis=-1, keepdims=True)

    products = pairs * jnp.concatenate([pairs[:, part:], pairs[:, :part]], axis=1)
    match = head_total(products) * 0.5
    readout = carried[...] * sums[...] + (weight[...] * match) * flat[:, lanes : 2 * lanes]
    scale = lax.rsqrt(head_total(readout * readout) / values + epsilon)
    gates = jax.nn.sigmoid(flat[:, 2 * lanes : 3 * lanes])
    mixed = readout * scale * gain[...] * gates
    for chip in range(chips):
        tile = mixed[chip * seqs : (chip + 1) * seqs, :].astype(bf16)
        for copy in range(chips):
            out[copy, :, chip * lanes : (chip + 1) * lanes] = tile


def pick_kernel(me, gate, same_routed, other_routed, same_tokens, other_tokens, pick, picked, gate_table, routed, rows, arrived):
    chips, seqs = same_tokens.shape[:2]
    half = chips * seqs
    core = me[0] % 2
    fetch = pltpu.make_async_copy(gate.at[0], gate_table, arrived)
    fetch.start()
    for chip in range(chips):
        at = chip * seqs
        routed[at : at + seqs, :] = same_routed[chip].astype(f32)
        routed[half + at : half + at + seqs, :] = other_routed[chip].astype(f32)
        rows[at : at + seqs, :] = same_tokens[chip].astype(f32)
        rows[half + at : half + at + seqs, :] = other_tokens[chip].astype(f32)
    choices = routed[...].T[:8]
    valid = lax.broadcasted_iota(jnp.int32, choices.shape, 0) < seqs
    hits = jnp.where(valid & (choices == me[0].astype(f32)), 1.0, 0.0)
    named = jnp.broadcast_to(jnp.sum(hits, axis=0, keepdims=True), hits.shape)
    lane = lax.broadcasted_iota(jnp.int32, hits.shape, 1)
    slot = jnp.zeros(hits.shape, f32)
    for back in range(1, seqs):
        slot = slot + jnp.where(lane % seqs >= back, pltpu.roll(named, back, 1), 0.0)
    source = 2 * (lane % half // seqs) + jnp.where(lane < half, core, 1 - core)
    place = jnp.where(named > 0.0, 2 * source + slot.astype(jnp.int32), -1)
    index = lax.broadcasted_iota(jnp.int32, pick.shape, 0)
    slots = 4 * chips
    mine = lax.broadcasted_iota(jnp.int32, pick.shape, 1) + slots - me[0] // 2 * seqs
    wanted = jnp.where(index < slots, jnp.broadcast_to(place[:1], pick.shape), mine)
    chosen = jnp.where(wanted == index, 1.0, 0.0).astype(bf16)
    pick[...] = chosen
    picked[...] = jnp.dot(chosen, rows[...].astype(bf16), preferred_element_type=f32).astype(bf16)
    fetch.wait()


def expert_kernel(pick, tokens, same, other, gain, gate_table, lift, down, out, own, branch, *refs):
    lift_table, down_table, arrived = refs
    copies = [
        pltpu.make_async_copy(source.at[0], target, arrived.at[i])
        for i, (source, target) in enumerate(
            ((lift, lift_table), (down, down_table))
        )
    ]
    for copy in copies:
        copy.start()
    chips, rows = same.shape[:2]
    for chip in range(chips):
        columns = slice(chip * lanes, (chip + 1) * lanes)
        branch[:rows, columns] = same[chip]
        branch[rows:, columns] = other[chip]
    added = jnp.dot(pick[...], branch[...], preferred_element_type=f32)
    residual = (tokens[...].astype(f32) + added).astype(bf16)
    devices, capacity = out.shape[:2]
    slots = devices * capacity
    own[...] = residual[slots:][: own.shape[0]]
    expert_in = scaled_norm(residual[:slots].astype(f32), gain[...]).astype(bf16)
    gate_value = jnp.dot(expert_in, gate_table[...], preferred_element_type=f32)
    copies[0].wait()
    lift_value = jnp.dot(expert_in, lift_table[...], preferred_element_type=f32)
    hidden = (jax.nn.silu(gate_value) * lift_value).astype(bf16)
    copies[1].wait()
    results = jnp.dot(hidden, down_table[...], preferred_element_type=f32)
    for device in range(devices):
        out[device] = results[device * capacity : (device + 1) * capacity, :].astype(bf16)


def combine_kernel(place, weights, returned, own, out, rows):
    seqs, choices = weights.shape
    devices, capacity = returned.shape[:2]
    for device in range(devices):
        rows[device * capacity : (device + 1) * capacity, :] = returned[device].astype(f32)
    lane = lax.broadcasted_iota(jnp.int32, (seqs, devices * capacity), 1)
    chosen = [
        jnp.where(lane == place[:, choice : choice + 1], 1.0, 0.0) for choice in range(choices)
    ]
    results = rows[...].astype(bf16)
    total = jnp.zeros(out.shape, f32)
    for choice in range(choices):
        picked = jnp.dot(chosen[choice].astype(bf16), results, preferred_element_type=f32)
        total = total + (weights[:, choice : choice + 1] * picked).astype(bf16).astype(f32)
    out[...] = (own[...].astype(f32) + total).astype(bf16)


def body(
    tokens,
    memory_state,
    max_state,
    norm_gain,
    query_weight,
    key_weight,
    value_weight,
    output_gate,
    input_gate,
    forget_gate,
    forget_bias,
    head_gain,
    output_weight,
    expert_norm,
    routed_experts,
    route_weights,
    expert_gate,
    expert_lift,
    expert_down,
):
    seq_rows, width = tokens.shape
    head_count = forget_bias.shape[0]
    key_size = memory_state.shape[2]
    value_size = memory_state.shape[3]
    axis_size = lax.axis_size("ep")
    chips = axis_size // 2
    me = lax.axis_index("ep")
    half_rows = chips * seq_rows
    capacity = min(seq_rows, 2)
    choices = routed_experts.shape[1]

    blocks = relay(tokens)
    assert sorted(at % chips for at in relay_order(0)) == list(range(chips))

    pairs = []
    for table in (query_weight, key_weight, value_weight, output_gate, output_weight):
        pairs += [table.T, partner(table.T)]
    total = sum(table.shape[0] for table in pairs[:-2])

    per_head = chips // head_count
    gate_shape = jax.ShapeDtypeStruct((seq_rows, head_count), f32)
    row_shape = jax.ShapeDtypeStruct((half_rows, lanes), f32)
    gate_inputs = (
        tokens,
        norm_gain[None],
        input_gate.T,
        forget_gate.T,
        forget_bias[None],
        max_state,
        head_gain.reshape(chips, lanes),
        routed_experts,
    )
    new_max, carried, written, carried_rows, weight_rows, gain_rows, routing = pl.pallas_call(
        lambda *refs: gate_kernel(key_size, *refs),
        out_shape=(gate_shape,) * 3
        + (row_shape,) * 3
        + (jax.ShapeDtypeStruct((seq_rows, lanes), bf16),),
        in_specs=[hbm] * 8,
        out_specs=(whole,) * 7,
        scratch_shapes=[pltpu.VMEM(array.shape, array.dtype) for array in gate_inputs]
        + [pltpu.SemaphoreType.DMA((8,))],
        compiler_params=pltpu.CompilerParams(vmem_limit_bytes=4 << 20),
        name="gates",
    )(*map(in_hbm, gate_inputs))
    blocks, theirs, carried_rows, weight_rows, gain_rows, routing = lax.optimization_barrier(
        (blocks, pairs[1::2], carried_rows, weight_rows, gain_rows, routing)
    )

    pairs[1::2] = theirs
    pairs[:-2:2] = map(in_hbm, pairs[:-2:2])
    projected, same_tokens = pl.pallas_call(
        project_kernel,
        out_shape=(
            jax.ShapeDtypeStruct((chips, seq_rows, total + lanes), bf16),
            jax.ShapeDtypeStruct((chips, seq_rows, width), bf16),
        ),
        in_specs=[scalar, whole, hbm] + [whole] * len(blocks) + [hbm, whole] * (len(pairs) // 2 - 1),
        out_specs=(whole, whole),
        scratch_shapes=[
            pltpu.VMEM((total, width), bf16),
            pltpu.VMEM((half_rows, width), f32),
            pltpu.VMEM((1, width), f32),
            pltpu.SemaphoreType.DMA((len(pairs) // 2,)),
        ],
        compiler_params=pltpu.CompilerParams(vmem_limit_bytes=8 << 20),
        name="project",
    )(me[None], routing, in_hbm(norm_gain[None]), *blocks, *pairs[:-2])
    received = exchange(projected)
    same_mixed = exchange(
        pl.pallas_call(
            readout_kernel,
            out_shape=jax.ShapeDtypeStruct((chips, seq_rows, width), bf16),
            in_specs=[pl.BlockSpec(memory_space=pltpu.HBM)] + [whole] * 4,
            out_specs=whole,
            scratch_shapes=[
                pltpu.VMEM((half_rows, lanes), f32),
                pltpu.VMEM((half_rows, total + lanes), f32),
                pltpu.VMEM(memory_state.shape, f32),
                pltpu.SemaphoreType.DMA(memory_state.shape[:2]),
            ],
            compiler_params=pltpu.CompilerParams(vmem_limit_bytes=48 << 20),
            name="readout",
        )(memory_state, received, carried_rows, weight_rows, gain_rows)
    )

    by_source = received
    edge = total // 6

    def own_columns(start, size):
        return (
            by_source[:, :, start : start + size]
            .transpose(1, 0, 2)
            .reshape(seq_rows, head_count, chips * size // head_count)
            .astype(f32)
        )

    key_heads = own_columns(edge, edge)
    value_heads = own_columns(2 * edge, 2 * edge)
    new_memory = (
        carried[:, :, None, None] * memory_state
        + (written[:, :, None] * key_heads)[:, :, :, None] * value_heads[:, :, None, :]
    )

    columns = pl.pallas_call(
        mix_kernel,
        out_shape=jax.ShapeDtypeStruct((chips, half_rows, lanes), bf16),
        in_specs=[scalar] + [whole] * 3,
        out_specs=whole,
        scratch_shapes=[pltpu.VMEM((lanes, width), bf16), pltpu.VMEM((half_rows, width), f32)],
        compiler_params=pltpu.CompilerParams(vmem_limit_bytes=4 << 20),
        name="mix",
    )(me[None], same_mixed, *pairs[-2:])
    same_branch = exchange(columns)
    slots = axis_size * capacity
    same_routed = received[:, :, total:]
    pick, picked_tokens, gate_table = pl.pallas_call(
        pick_kernel,
        out_shape=(
            jax.ShapeDtypeStruct((slots + 16, 2 * half_rows), bf16),
            jax.ShapeDtypeStruct((slots + 16, width), bf16),
            jax.ShapeDtypeStruct(expert_gate.shape[1:], bf16),
        ),
        in_specs=[scalar, hbm] + [whole] * 4,
        out_specs=(whole,) * 3,
        scratch_shapes=[
            pltpu.VMEM((2 * half_rows, lanes), f32),
            pltpu.VMEM((2 * half_rows, width), f32),
            pltpu.SemaphoreType.DMA(()),
        ],
        compiler_params=pltpu.CompilerParams(vmem_limit_bytes=8 << 20),
        name="pick",
    )(me[None], in_hbm(expert_gate), same_routed, partner(same_routed), same_tokens, partner(same_tokens))
    picked_tokens, pick, gate_table, same_branch = lax.optimization_barrier(
        (picked_tokens, pick, gate_table, same_branch)
    )
    results, own_residual = pl.pallas_call(
        expert_kernel,
        out_shape=(
            jax.ShapeDtypeStruct((axis_size, capacity, width), bf16),
            jax.ShapeDtypeStruct((seq_rows, width), bf16),
        ),
        in_specs=[whole] * 6 + [hbm] * 2,
        out_specs=(whole, whole),
        scratch_shapes=[
            pltpu.VMEM((2 * half_rows, width), bf16),
            pltpu.VMEM(expert_lift.shape[1:], bf16),
            pltpu.VMEM(expert_down.shape[1:], bf16),
            pltpu.SemaphoreType.DMA((2,)),
        ],
        compiler_params=pltpu.CompilerParams(vmem_limit_bytes=24 << 20),
        name="experts",
    )(
        pick,
        picked_tokens,
        same_branch,
        partner(same_branch),
        expert_norm[None],
        gate_table,
        *map(in_hbm, (expert_lift, expert_down)),
    )
    routed_experts, results = lax.optimization_barrier((routed_experts, results))
    returned = lax.all_to_all(results, "ep", split_axis=0, concat_axis=0, tiled=True)
    earlier = jnp.arange(seq_rows)[:, None] > jnp.arange(seq_rows)[None, :]
    same = routed_experts[:, :, None, None] == routed_experts[None, None, :, :]
    slot_index = jnp.sum(
        (same & earlier[:, None, :, None]).astype(jnp.int32), axis=(2, 3), dtype=jnp.int32
    )
    layer_out = pl.pallas_call(
        combine_kernel,
        out_shape=jax.ShapeDtypeStruct((seq_rows, width), bf16),
        in_specs=[whole] * 4,
        out_specs=whole,
        scratch_shapes=[pltpu.VMEM((slots, width), f32)],
        compiler_params=pltpu.CompilerParams(vmem_limit_bytes=4 << 20),
        name="combine",
    )(routed_experts * capacity + slot_index, route_weights, returned, own_residual)
    return (layer_out, new_memory, new_max)


def solution(mesh):
    return jax.shard_map(
        body,
        mesh=mesh,
        in_specs=(
            P(("grp", "ep"), None),
            P(("grp", "ep"), None, None, None),
            P(("grp", "ep"), None),
            P(),
            P(None, "ep"),
            P(None, "ep"),
            P(None, "ep"),
            P(None, "ep"),
            P(),
            P(),
            P(),
            P(),
            P(None, "ep"),
            P(),
            P(("grp", "ep"), None),
            P(("grp", "ep"), None),
            P("ep", None, None),
            P("ep", None, None),
            P("ep", None, None),
        ),
        out_specs=(
            P(("grp", "ep"), None),
            P(("grp", "ep"), None, None, None),
            P(("grp", "ep"), None),
        ),
        check_vma=False,
    )
```
